512 devices in a mesh: kv: 16 (over y, x), tp: 32 (over z, core).
Axes of the slice: x: 4, y: 4, z: 16, core: 2. Of those that a mesh axis runs over, the one named last changes fastest.
Arguments:
- tokens: bfloat16 [16, 4096], P(None, ('kv', 'tp')), may hold values from -8 to 8
- attention_gain: bfloat16 [4096], replicated, may hold values from 0.099609375 to 1.8984375
- query_weight: bfloat16 [2048, 4096], P('tp', 'kv'), may hold values from -0.09375 to 0.09375
- key_weight: bfloat16 [2048, 4096], P('tp', 'kv'), may hold values from -0.09375 to 0.09375
- value_weight: bfloat16 [2048, 4096], P('tp', 'kv'), may hold values from -0.09375 to 0.09375
- forget_weight: bfloat16 [32, 4096], replicated, may hold values from -0.09375 to 0.09375
- cached_pairs: bfloat16 [16, 32, 2, 64, 16384], P(None, 'tp', None, None, 'kv'), may hold values from -200 to 200
- cached_gates: float32 [16, 32, 16384], P(None, 'tp', 'kv'), as said below
- lengths: int32 [16], replicated, may hold values from 1 to 16384, as said below
- output_weight: bfloat16 [2048, 4096], P('tp', 'kv'), may hold values from -1.5 to 1.5
- mixer_gain: bfloat16 [4096], replicated, may hold values from 0.099609375 to 1.8984375
- up_weight: bfloat16 [16384, 4096], P('tp', 'kv'), may hold values from -0.09375 to 0.09375
- down_weight: bfloat16 [16384, 4096], P('tp', 'kv'), may hold values from -0.09375 to 0.09375
Outputs:
- mixed: bfloat16 [16, 4096], P(None, ('kv', 'tp'))
The draws below stay inside these ranges and needn't reach their ends.
Inputs may be any that keep to these rules, and one draw needn't show every extreme that they name: `cached_gates`: below a sequence's length, the sum of the log forget gates of the later live cached positions of that sequence and head; zero at and beyond the length. `lengths`: in every draw one sequence has length 16384.
All inputs are finite; a program needn't handle non-finite values.
Results may differ from the reference program's by a relative error of at most 0.015.
Values may be sent and summed in bfloat16 or wider, within the bound.
No kernel may reach another device: no remote copies, remote signals or barrier semaphores. Data moves between devices by JAX's collectives and lax.ppermute only.
A program may use at most 64 MiB of HBM per device.

```python
import jax
import jax.numpy as jnp
from jax import lax

D = 4096
ATTENDER_NUMBER = 32
HD = 64
FF = 16384
BATCH_STRINGS = 16
POS_DEV = 1024
STORED_SPAN = 16384
N_KV = 16


def seq_lengths(key):
    base = jax.random.fold_in(key, 11)
    first, second = jax.random.split(base)
    picks = jax.random.randint(first, (BATCH_STRINGS,), 0, 1024)
    spread = (STORED_SPAN - 1) * (picks * picks // 1024) // 1024
    longest = jax.random.randint(second, (), 0, BATCH_STRINGS)
    return jnp.where(jnp.arange(BATCH_STRINGS) == longest, STORED_SPAN, 1 + spread).astype(jnp.int32)


def draw_lengths(key, part):
    return seq_lengths(key)


def draw_tokens(key, part):
    address_items = jax.random.split(key, 4)
    columns = jnp.arange(D, dtype=jnp.float32) / D
    rough = jax.random.uniform(address_items[0], (D,), jnp.float32, 0.6, 1.6)
    column_scale = 0.6 * jnp.exp(columns * jnp.log(4.0)) * rough
    values = jax.random.normal(address_items[1], (BATCH_STRINGS, D), jnp.float32)
    row_scale = jnp.exp(jax.random.uniform(address_items[3], (BATCH_STRINGS, 1), jnp.float32, jnp.log(0.5), jnp.log(2.0)))
    return jnp.clip(values * row_scale * column_scale, -8.0, 8.0).astype(jnp.bfloat16)


def draw_cached_pairs(key, part):

    def one_sequence(number):
        sub = jax.random.fold_in(key, number)
        first = jax.random.fold_in(sub, 0)
        values = jnp.clip(jax.random.normal(first, (ATTENDER_NUMBER, 2, HD, STORED_SPAN), jnp.float32), -5.0, 5.0)
        return values.astype(jnp.bfloat16)
    return lax.map(one_sequence, jnp.arange(BATCH_STRINGS))


def draw_cached_gates(key, part):
    live_lengths = seq_lengths(key)
    base = jax.random.fold_in(key, 23)
    address_items = jax.random.split(base, 5)
    order = jax.random.permutation(address_items[0], ATTENDER_NUMBER)
    trailing_attenders = order < ATTENDER_NUMBER // 2
    noise = jax.random.uniform(address_items[2], (BATCH_STRINGS, ATTENDER_NUMBER, STORED_SPAN), jnp.float32, 0.3, 1.7)
    rates = jnp.where(trailing_attenders, 0.5 / STORED_SPAN, 1.0 / 25.0)
    factor = jnp.exp(jax.random.uniform(address_items[1], (BATCH_STRINGS, ATTENDER_NUMBER, STORED_SPAN // POS_DEV), jnp.float32, jnp.log(0.5), jnp.log(2.0)))
    factor = jnp.repeat(factor, POS_DEV, axis=2)
    stride_additions = -rates[None, :, None] * factor * noise
    packet_clusters = (jax.random.randint(address_items[3], (BATCH_STRINGS, ATTENDER_NUMBER, STORED_SPAN), 0, STORED_SPAN) < 2) & trailing_attenders[None, :, None]
    penalty_figures = jnp.log(jax.random.uniform(address_items[4], (BATCH_STRINGS, ATTENDER_NUMBER, STORED_SPAN), jnp.float32, 0.5, 0.8))
    stride_additions = stride_additions + jnp.where(packet_clusters, penalty_figures, 0.0)
    totals = jnp.cumsum(stride_additions, axis=2)
    last_index = jnp.broadcast_to((live_lengths - 1)[:, None, None], (BATCH_STRINGS, ATTENDER_NUMBER, 1))
    last_total = jnp.take_along_axis(totals, last_index, axis=2)
    live_mask = jnp.arange(STORED_SPAN)[None, None, :] < live_lengths[:, None, None]
    return jnp.where(live_mask, last_total - totals, 0.0)


def raised(values, key, source, target, blocks, factor):
    owner, partner = [(jnp.arange(values.shape[position]) // (values.shape[position] // blocks)).reshape([-1 if axis == position else 1 for axis in range(values.ndim)]) for position in (source, target)]
    chosen = jax.random.permutation(key, blocks)[partner]
    strong = (owner == chosen) | (owner == (partner + blocks // 2) % blocks)
    return jnp.where(strong, factor * values, values)


def block_levels(stream_key, shape, cuts, low, top_value):
    def one(position, parts):
        steps = jax.random.uniform(jax.random.fold_in(jax.random.fold_in(stream_key, 6), position), (parts,), jnp.float32, low / len(cuts), top_value / len(cuts))
        return jnp.repeat(jnp.exp(steps), shape[position] // parts).reshape((-1,) + (1,) * (len(shape) - position - 1))

    gain = one(*cuts[0])
    for cut in cuts[1:]:
        gain = gain * one(*cut)
    return gain


def normal_values(key, shape, deviation, bound, shards=(), held_as=jnp.bfloat16):
    result = deviation * jax.random.normal(key, shape, jnp.float32)
    if shards:
        result = result * block_levels(key, shape, shards, -0.22, 0.18)
    return jnp.clip(result, -bound, bound).astype(held_as)


def bell_draw_with(stream_key, shape, deviation, bound, cuts, heavy, kind=jnp.bfloat16):
    entries = deviation * jax.random.normal(stream_key, shape, jnp.float32)
    if cuts:
        entries = entries * block_levels(stream_key, shape, cuts, -0.22, 0.18)
    return jnp.clip(raised(entries, jax.random.fold_in(stream_key, 3), *heavy), -bound, bound).astype(kind)


def setup_inputs(seed: int = 0) -> dict:
    keys = jax.random.split(jax.random.key(seed), 14)
    return {
        "tokens": draw_tokens(jax.random.fold_in(keys[13], 71), 0),
        "attention_gain": jnp.clip(1.0 + 0.18 * jax.random.normal(keys[1], (D,), jnp.float32), 0.099609375, 1.8984375).astype(jnp.bfloat16),
        "query_weight": normal_values(keys[2], (ATTENDER_NUMBER * HD, D), D ** -0.5, 0.09375, ((0, 32), (1, 16))),
        "key_weight": normal_values(keys[3], (ATTENDER_NUMBER * HD, D), D ** -0.5, 0.09375, ((0, 32), (1, 16))),
        "value_weight": normal_values(keys[4], (ATTENDER_NUMBER * HD, D), D ** -0.5, 0.09375, ((0, 32), (1, 16))),
        "forget_weight": normal_values(keys[5], (ATTENDER_NUMBER, D), D ** -0.5, 0.09375),
        "cached_pairs": draw_cached_pairs(jax.random.fold_in(keys[13], 71), 0),
        "cached_gates": draw_cached_gates(jax.random.fold_in(keys[13], 71), 0),
        "lengths": draw_lengths(jax.random.fold_in(keys[13], 71), 0),
        "output_weight": bell_draw_with(keys[9], (ATTENDER_NUMBER * HD, D), HD ** -0.5, 1.5, ((0, 32), (1, 16)), (0, 1, 32, 2.75)),
        "mixer_gain": jnp.clip(1.0 + 0.18 * jax.random.normal(keys[10], (D,), jnp.float32), 0.099609375, 1.8984375).astype(jnp.bfloat16),
        "up_weight": normal_values(keys[11], (FF, D), D ** -0.5, 0.09375, ((0, 32), (1, 16))),
        "down_weight": bell_draw_with(keys[12], (FF, D), FF ** -0.5, 0.09375, ((0, 32), (1, 16)), (0, 1, 32, 2.75)),
    }


EPSILON = 1e-06
NEG_FILL = -1e+30

def reference(tokens, attention_gain, query_weight, key_weight, value_weight, forget_weight, cached_pairs, cached_gates, lengths, output_weight, mixer_gain, up_weight, down_weight):
    token_float = tokens.astype(jnp.float32)
    row_scale = lax.rsqrt(lax.optimization_barrier(jnp.mean(token_float * token_float, axis=1, keepdims=True)) + EPSILON)
    scaled_rows = (token_float * attention_gain.astype(jnp.float32)).astype(jnp.bfloat16)

    def project(weight):
        return jnp.dot(scaled_rows, weight.T, preferred_element_type=jnp.float32) * row_scale
    query_rows = project(query_weight).astype(jnp.bfloat16).reshape(BATCH_STRINGS, ATTENDER_NUMBER, HD)
    key_rows = project(key_weight).astype(jnp.bfloat16).reshape(BATCH_STRINGS, ATTENDER_NUMBER, HD)
    value_rows = project(value_weight).astype(jnp.bfloat16).reshape(BATCH_STRINGS, ATTENDER_NUMBER, HD)
    forget = jax.nn.log_sigmoid(project(forget_weight))
    live_mask = jnp.arange(STORED_SPAN)[None, :] < lengths[:, None]
    block_mask = live_mask.reshape(BATCH_STRINGS, N_KV, POS_DEV)
    score_scale = HD ** (-0.5)

    def one_head(head_number):
        keys_float = cached_pairs[:, head_number, 0].astype(jnp.float32)
        values_float = cached_pairs[:, head_number, 1].astype(jnp.float32)
        query_float = query_rows[:, head_number].astype(jnp.float32)
        raw_scores = jnp.einsum('sd,sdl->sl', query_float, keys_float) * score_scale
        scores = jnp.where(live_mask, raw_scores + cached_gates[:, head_number] + forget[:, head_number][:, None], NEG_FILL)
        blocked = scores.reshape(BATCH_STRINGS, N_KV, POS_DEV)
        block_top = lax.optimization_barrier(jnp.max(blocked, axis=2))
        weights = jnp.where(block_mask, jnp.exp(blocked - block_top[..., None]), 0.0)
        block_total = lax.optimization_barrier(jnp.sum(weights, axis=2))
        rounded = lax.optimization_barrier(weights.astype(jnp.bfloat16)).astype(jnp.float32)
        block_sum = jnp.einsum('snp,sdnp->snd', rounded, values_float.reshape(BATCH_STRINGS, HD, N_KV, POS_DEV))
        own_score = lax.optimization_barrier(jnp.sum(query_float * key_rows[:, head_number].astype(jnp.float32), axis=1)) * score_scale
        highest = jnp.maximum(lax.optimization_barrier(jnp.max(block_top, axis=1)), own_score)
        cache_factor = jnp.exp(block_top - highest[:, None])
        own_factor = jnp.exp(own_score - highest)
        numerator = lax.optimization_barrier(jnp.sum(cache_factor[..., None] * block_sum, axis=1)) + own_factor[:, None] * value_rows[:, head_number].astype(jnp.float32)
        denominator = lax.optimization_barrier(jnp.sum(cache_factor * block_total, axis=1)) + own_factor
        return (numerator / denominator[:, None]).astype(jnp.bfloat16)
    attended = lax.map(one_head, jnp.arange(ATTENDER_NUMBER))
    attended = jnp.transpose(attended, (1, 0, 2)).reshape(BATCH_STRINGS, ATTENDER_NUMBER * HD)
    attention_out = jnp.dot(attended, output_weight, preferred_element_type=jnp.float32)
    middle = (token_float + attention_out).astype(jnp.bfloat16)
    middle_float = middle.astype(jnp.float32)
    middle_scale = lax.rsqrt(lax.optimization_barrier(jnp.mean(middle_float * middle_float, axis=1, keepdims=True)) + EPSILON)
    scaled_middle = (middle_float * mixer_gain.astype(jnp.float32)).astype(jnp.bfloat16)
    hidden_pre = jnp.dot(scaled_middle, up_weight.T, preferred_element_type=jnp.float32) * middle_scale
    activated = jnp.square(jax.nn.relu(hidden_pre)).astype(jnp.bfloat16)
    down_out = jnp.dot(activated, down_weight, preferred_element_type=jnp.float32)
    return (middle_float + down_out).astype(jnp.bfloat16)
```

```python
import jax
import jax.numpy as jnp
from jax import lax
from jax.sharding import Mesh
from jax.sharding import PartitionSpec as P

HD = 64
KV = ("kv_0", "kv_1")
TP = ("z", "core")
KV_TP = (*KV, *TP)

EPSILON = 1e-06
NEG_FILL = -1e30


def copy_for_each(array, axes):
    copies = jnp.broadcast_to(array, (lax.axis_size(axes), *array.shape))
    return lax.all_to_all(copies, axes, split_axis=0, concat_axis=0, tiled=True)


def contract(left_rows, weight_rows):
    return lax.dot_general(
        left_rows, weight_rows, (((1,), (1,)), ((), ())), preferred_element_type=jnp.float32
    )


def lanes(parts, width):
    joined = jnp.concatenate(parts, axis=1)
    return jnp.pad(joined, ((0, 0), (0, width - joined.shape[1])))


def local(
    tokens,
    attention_gain,
    query_weight,
    key_weight,
    value_weight,
    forget_weight,
    cached_pairs,
    cached_gates,
    lengths,
    output_weight,
    mixer_gain,
    up_weight,
    down_weight,
):
    position_index = lax.axis_index(KV)
    head_index = lax.axis_index(TP)
    sequences, own_columns = tokens.shape
    block_columns = query_weight.shape[1]
    model_width = block_columns * lax.axis_size(KV)
    position_count = cached_pairs.shape[-1]

    gathered = copy_for_each(tokens, TP)
    block_float = jnp.moveaxis(gathered, 0, 1).reshape(sequences, -1).astype(jnp.float32)
    start = position_index * block_columns
    block_gain = lax.dynamic_slice_in_dim(attention_gain, start, block_columns, 0)
    own_block = (block_float * block_gain.astype(jnp.float32)).astype(jnp.bfloat16)
    forget_row = lax.dynamic_slice(forget_weight, (head_index, start), (1, block_columns))
    query_part = contract(own_block, query_weight)
    key_part = contract(own_block, key_weight)
    value_part = contract(own_block, value_weight)
    forget_part = contract(own_block, forget_row)
    squares_part = jnp.sum(block_float * block_float, axis=1, keepdims=True)

    first = copy_for_each(lanes([query_part, forget_part, squares_part], 128), KV)
    first = jnp.sum(first, axis=0)
    scale_rows = lax.rsqrt(first[:, HD + 1 : HD + 2] / model_width + EPSILON)
    query = (first[:, :HD] * scale_rows).astype(jnp.bfloat16)
    forget = jax.nn.log_sigmoid(first[:, HD : HD + 1] * scale_rows)
    score_scale = HD ** (-0.5)
    own_part = jnp.sum(query.astype(jnp.float32) * key_part, axis=1, keepdims=True)

    positions = position_index * position_count + jnp.arange(position_count)
    live_mask = positions[None, :] < lengths[:, None]
    raw_scores = jnp.einsum(
        "sd,sdp->sp", query, cached_pairs[:, 0, 0], preferred_element_type=jnp.float32
    )
    scores = jnp.where(live_mask, raw_scores * score_scale + cached_gates[:, 0], NEG_FILL)
    block_top = jnp.max(scores, axis=1, keepdims=True)
    weights = jnp.where(live_mask, jnp.exp(scores - block_top), 0.0)
    block_total = jnp.sum(weights, axis=1, keepdims=True)
    block_sum = jnp.einsum(
        "sp,sdp->sd",
        weights.astype(jnp.bfloat16),
        cached_pairs[:, 0, 1],
        preferred_element_type=jnp.float32,
    )

    second = copy_for_each(
        lanes([block_sum, value_part, block_top, block_total, own_part], 256), KV
    )
    tops = second[:, :, 2 * HD] + forget[:, 0][None]
    own_score = jnp.sum(second[:, :, 2 * HD + 2], axis=0) * scale_rows[:, 0] * score_scale
    value_new = jnp.sum(second[:, :, HD : 2 * HD], axis=0) * scale_rows
    value_new = value_new.astype(jnp.bfloat16).astype(jnp.float32)
    highest = jnp.maximum(jnp.max(tops, axis=0), own_score)
    factors = jnp.exp(tops - highest[None])
    own_factor = jnp.exp(own_score - highest)
    numerator = jnp.sum(factors[..., None] * second[:, :, :HD], axis=0)
    numerator = numerator + own_factor[:, None] * value_new
    denominator = jnp.sum(factors * second[:, :, 2 * HD + 1], axis=0) + own_factor
    attended = (numerator / denominator[:, None]).astype(jnp.bfloat16)

    projected = jnp.dot(attended, output_weight, preferred_element_type=jnp.float32)
    projected = jnp.sum(copy_for_each(projected, "core"), axis=0).astype(jnp.bfloat16)
    projected = jnp.sum(copy_for_each(projected, "z").astype(jnp.float32), axis=0)
    middle = (block_float + projected).astype(jnp.bfloat16)
    middle_float = middle.astype(jnp.float32)
    middle_gain = lax.dynamic_slice_in_dim(mixer_gain, start, block_columns, 0)
    scaled_middle = (middle_float * middle_gain.astype(jnp.float32)).astype(jnp.bfloat16)

    hidden_part = contract(scaled_middle, up_weight)
    hidden_units = hidden_part.shape[1]
    middle_squares = jnp.sum(middle_float * middle_float, axis=1, keepdims=True)
    third = lanes([hidden_part, middle_squares], hidden_units + 128).astype(jnp.bfloat16)
    third = jnp.sum(copy_for_each(third, KV).astype(jnp.float32), axis=0)
    middle_scale = lax.rsqrt(third[:, hidden_units : hidden_units + 1] / model_width + EPSILON)
    activated = jnp.square(jax.nn.relu(third[:, :hidden_units] * middle_scale)).astype(jnp.bfloat16)

    down_term = jnp.dot(activated, down_weight, preferred_element_type=jnp.float32)
    tiles = jnp.moveaxis(down_term.reshape(sequences, -1, own_columns), 1, 0)
    tiles = lax.all_to_all(tiles, TP, 0, 0, tiled=True)
    middle_own = lax.dynamic_slice_in_dim(middle_float, head_index * own_columns, own_columns, 1)
    return (middle_own + jnp.sum(tiles, axis=0)).astype(jnp.bfloat16)


def solution(mesh):
    split = Mesh(mesh.devices.reshape(4, 4, 16, 2), KV_TP)
    return jax.shard_map(
        local,
        mesh=split,
        in_specs=(
            P(None, KV_TP),
            P(),
            P(TP, KV),
            P(TP, KV),
            P(TP, KV),
            P(),
            P(None, TP, None, None, KV),
            P(None, TP, KV),
            P(),
            P(TP, KV),
            P(),
            P(TP, KV),
            P(TP, KV),
        ),
        out_specs=P(None, KV_TP),
        check_vma=False,
    )
```

```python
import functools

import jax
import jax.numpy as jnp
from jax import lax
from jax.experimental import pallas as pl
from jax.experimental.pallas import tpu as pltpu
from jax.sharding import Mesh
from jax.sharding import PartitionSpec as P

HD = 64
KV = ("kv_0", "kv_1")
TP = ("z", "core")
KV_TP = (*KV, *TP)
LANES = 128

COST = 1 << 34
EPSILON = 1e-06
NEG_FILL = -1e30
F32 = jnp.float32
BF16 = jnp.bfloat16


def exchange(copies, axes):
    return lax.all_to_all(copies, axes, split_axis=0, concat_axis=0, tiled=True)


def near(array):
    return pltpu.with_memory_space_constraint(array, pltpu.VMEM)


def call(body, outs, name, scratch=()):
    return pl.pallas_call(
        body,
        out_shape=[jax.ShapeDtypeStruct(shape, dtype) for shape, dtype in outs],
        scratch_shapes=list(scratch),
        name=name,
        cost_estimate=pl.CostEstimate(flops=COST, bytes_accessed=COST // 256, transcendentals=0),
        compiler_params=pltpu.CompilerParams(vmem_limit_bytes=24 << 20),
    )


def rows_dot(left, right):
    return lax.dot_general(left, right, (((1,), (1,)), ((), ())), preferred_element_type=F32)


def iota(shape, dim):
    return lax.broadcasted_iota(jnp.int32, shape, dim)


def block_gain(gain_ref, block):
    gains = gain_ref[...].astype(F32)
    rows = iota(gains.shape, 0)
    first = jnp.sum(jnp.where(rows == 2 * block, gains, 0.0), axis=0, keepdims=True)
    second = jnp.sum(jnp.where(rows == 2 * block + 1, gains, 0.0), axis=0, keepdims=True)
    return jnp.concatenate([first, second], axis=1)


def spread_body(tokens, out):
    rows = tokens[...].astype(F32)
    line = jnp.concatenate([rows[at : at + 1] for at in range(rows.shape[0])], axis=1)
    out[...] = jnp.broadcast_to(line[None], out.shape)


def project_body(got, gain, query_w, key_w, value_w, forget_w, first_out, parts_out, block_out):
    position = lax.axis_index("kv_0") * 4 + lax.axis_index("kv_1")
    head = lax.axis_index("z") * 2 + lax.axis_index("core")
    peers = got.shape[0]
    sequences = block_out.shape[0]
    columns = LANES // sequences
    spread = jnp.broadcast_to(got[...], (peers, columns, LANES)).reshape(peers * columns, LANES)
    keep = (iota(spread.shape, 1) // sequences) == (iota(spread.shape, 0) % columns)
    fold = (iota((sequences, LANES), 1) % sequences) == iota((sequences, LANES), 0)
    block = rows_dot(
        jnp.where(fold, 1.0, 0.0).astype(BF16), jnp.where(keep, spread, 0.0).astype(BF16)
    )
    block_out[...] = block
    own = (block * block_gain(gain, position)).astype(BF16)
    query = rows_dot(own, query_w[...])
    key = rows_dot(own, key_w[...])
    value = rows_dot(own, value_w[...])
    width = block.shape[1]
    gate_rows = forget_w[:, pl.ds(pl.multiple_of(position * width, width), width)]
    gates = rows_dot(own, gate_rows)
    gate = jnp.sum(jnp.where(iota(gates.shape, 1) == head, gates, 0.0), axis=1, keepdims=True)
    squares = jnp.sum(block * block, axis=1, keepdims=True)
    lane = iota((sequences, LANES - HD), 1)
    rest = jnp.where(lane == 0, gate, jnp.where(lane == 1, squares, 0.0))
    line = jnp.concatenate([query, rest], axis=1)
    first_out[...] = jnp.broadcast_to(line[None], first_out.shape)
    parts_out[...] = jnp.concatenate([key, value], axis=1)


def pieces(column):
    high = column.astype(BF16).astype(F32)
    middle = (column - high).astype(BF16).astype(F32)
    return high, middle, column - high - middle


def attend_body(model_width, got, parts, pairs, gates, lengths, second_out, row_out):
    position = lax.axis_index("kv_0") * 4 + lax.axis_index("kv_1")
    sequences = parts.shape[0]
    count = gates.shape[2]
    line = jnp.sum(got[...], axis=0)
    scale = lax.rsqrt(line[:, HD + 1 : HD + 2] / model_width + EPSILON)
    query = (line[:, :HD] * scale).astype(BF16)
    forget = jax.nn.log_sigmoid(line[:, HD : HD + 1] * scale)
    wide = sequences * HD
    own_group = (iota((sequences, wide), 1) // HD) == iota((sequences, wide), 0)
    spread = jnp.concatenate([query.astype(F32)] * sequences, axis=1)
    spread = jnp.where(own_group, spread, 0.0).astype(BF16)
    keys = pairs[:, 0, 0].reshape(wide, count)
    raw = jnp.dot(spread, keys, preferred_element_type=F32)
    diagonal = iota((sequences, sequences), 0) == iota((sequences, sequences), 1)
    ends = jnp.broadcast_to(lengths[...].reshape(1, sequences), (sequences, sequences))
    ends = jnp.sum(jnp.where(diagonal, ends, 0), axis=1, keepdims=True) - position * count
    live = iota((sequences, count), 1) < ends
    scores = jnp.where(live, raw * HD ** (-0.5) + gates[:, 0, :], NEG_FILL)
    top = jnp.max(scores, axis=1, keepdims=True)
    weights = jnp.where(live, jnp.exp(scores - top), 0.0)
    total = jnp.sum(weights, axis=1, keepdims=True)
    values = pairs[:, 0, 1].reshape(wide, count)
    sums = jnp.where(own_group, rows_dot(weights.astype(BF16), values), 0.0)
    folded = sums[:, :LANES]
    for at in range(LANES, wide, LANES):
        folded = folded + sums[:, at : at + LANES]
    block_sum = folded[:, :HD] + folded[:, HD:]
    own = jnp.sum(query.astype(F32) * parts[:, :HD], axis=1, keepdims=True)
    lane = iota((sequences, LANES), 1)
    stats = jnp.zeros((sequences, LANES), F32)
    for at, piece in enumerate((*pieces(top), *pieces(total), *pieces(own))):
        stats = jnp.where(lane == at, piece, stats)
    out = jnp.concatenate([block_sum, parts[:, HD:], stats], axis=1).astype(BF16)
    second_out[...] = jnp.broadcast_to(out[None], second_out.shape)
    row_out[...] = jnp.where(lane == 0, forget, jnp.where(lane == 1, scale, 0.0))


def combine_body(got, row, output_w, out):
    sums = got[:, :, :HD].astype(F32)
    value_parts = got[:, :, HD:LANES].astype(F32)
    stats = got[:, :, LANES:].astype(F32)
    forget, scale = row[:, 0:1], row[:, 1:2]

    def stat(at):
        return stats[:, :, at : at + 1] + stats[:, :, at + 1 : at + 2] + stats[:, :, at + 2 : at + 3]

    tops = stat(0) + forget[None]
    own_score = jnp.sum(stat(6), axis=0) * scale * HD ** (-0.5)
    value_new = (jnp.sum(value_parts, axis=0) * scale).astype(BF16).astype(F32)
    highest = jnp.maximum(jnp.max(tops, axis=0), own_score)
    factors = jnp.exp(tops - highest[None])
    own_factor = jnp.exp(own_score - highest)
    numerator = jnp.sum(factors * sums, axis=0) + own_factor * value_new
    denominator = jnp.sum(factors * stat(3), axis=0) + own_factor
    attended = (numerator / denominator).astype(BF16)
    projected = jnp.dot(attended, output_w[...], preferred_element_type=F32)
    out[...] = jnp.broadcast_to(projected[None], out.shape)


def mix_body(got, block, gain, up_w, third_out, middle_out):
    position = lax.axis_index("kv_0") * 4 + lax.axis_index("kv_1")
    projected = jnp.sum(got[...].astype(F32), axis=0)
    middle = (block[...] + projected).astype(BF16)
    middle_out[...] = middle
    wide = middle.astype(F32)
    scaled = (wide * block_gain(gain, position)).astype(BF16)
    hidden = rows_dot(scaled, up_w[...])
    squares = jnp.sum(wide * wide, axis=1, keepdims=True)
    lane = iota((wide.shape[0], LANES), 1)
    stats = jnp.zeros(lane.shape, F32)
    for at, piece in enumerate(pieces(squares)):
        stats = jnp.where(lane == at, piece, stats)
    out = jnp.concatenate([hidden, stats], axis=1).astype(BF16)
    third_out[...] = jnp.broadcast_to(out[None], third_out.shape)


def down_body(model_width, got, down_w, out, turned):
    summed = jnp.sum(got[...].astype(F32), axis=0)
    units = down_w.shape[0]
    squares = summed[:, units : units + 1] + summed[:, units + 1 : units + 2]
    squares = squares + summed[:, units + 2 : units + 3]
    scale = lax.rsqrt(squares / model_width + EPSILON)
    activated = jnp.square(jax.nn.relu(summed[:, :units] * scale)).astype(BF16)
    sequences = activated.shape[0]
    down = jnp.dot(activated, down_w[...], preferred_element_type=F32)
    turned[...] = down.T
    peers = out.shape[0]
    columns = LANES // sequences
    lines = [turned[pl.ds(at, peers, stride=columns), :] for at in range(columns)]
    out[...] = jnp.concatenate(lines, axis=1).reshape(out.shape)


def finish_body(got, middle, out):
    head = lax.axis_index("z") * 2 + lax.axis_index("core")
    columns, sequences = out.shape
    line = jnp.sum(got[...], axis=0)
    own_shape = (columns, middle.shape[1])
    chosen = iota(own_shape, 1) == iota(own_shape, 0) + head * columns
    own = rows_dot(jnp.where(chosen, 1.0, 0.0).astype(BF16), middle[...])
    down = jnp.concatenate(
        [line[:, at * sequences : (at + 1) * sequences] for at in range(columns)], axis=0
    )
    out[...] = (own + down).astype(BF16)


def local(
    tokens,
    attention_gain,
    query_weight,
    key_weight,
    value_weight,
    forget_weight,
    cached_pairs,
    cached_gates,
    lengths,
    output_weight,
    mixer_gain,
    up_weight,
    down_weight,
):
    sequences, own_columns = tokens.shape
    blocks, heads = lax.axis_size(KV), lax.axis_size(TP)
    width = query_weight.shape[1]
    model_width = width * blocks
    hidden_units = up_weight.shape[0]

    (line,) = call(spread_body, [((heads, 1, sequences * own_columns), F32)], "spread")(tokens.T)
    got = exchange(line, TP)
    first, parts, block = call(
        project_body,
        [((blocks, sequences, LANES), F32), ((sequences, LANES), F32), ((sequences, width), F32)],
        "project",
    )(
        got,
        near(attention_gain.reshape(-1, LANES)),
        near(query_weight),
        near(key_weight),
        near(value_weight),
        near(forget_weight),
    )
    got = exchange(first, KV)
    second, row = call(
        functools.partial(attend_body, model_width),
        [((blocks, sequences, 2 * LANES), BF16), ((sequences, LANES), F32)],
        "attend",
    )(got, parts, near(cached_pairs), near(cached_gates), near(lengths))
    got = exchange(second, KV)
    (projected,) = call(combine_body, [((2, sequences, width), F32)], "combine")(
        got, row, near(output_weight)
    )
    projected = jnp.sum(exchange(projected, "core"), axis=0).astype(BF16)
    got = exchange(jnp.broadcast_to(projected, (lax.axis_size("z"), *projected.shape)), "z")
    third, middle = call(
        mix_body,
        [((blocks, sequences, hidden_units + LANES), BF16), ((sequences, width), BF16)],
        "mix",
    )(got, block, near(mixer_gain.reshape(-1, LANES)), near(up_weight))
    got = exchange(third, KV)
    (down,) = call(
        functools.partial(down_body, model_width),
        [((heads, 1, LANES), F32)],
        "down",
        [pltpu.VMEM((width, sequences), F32)],
    )(got, near(down_weight))
    got = exchange(down, TP)
    (out,) = call(finish_body, [((own_columns, sequences), BF16)], "finish")(got, middle)
    return out.T


def solution(mesh):
    split = Mesh(mesh.devices.reshape(4, 4, 16, 2), KV_TP)
    return jax.shard_map(
        local,
        mesh=split,
        in_specs=(
            P(None, KV_TP),
            P(),
            P(TP, KV),
            P(TP, KV),
            P(TP, KV),
            P(),
            P(None, TP, None, None, KV),
            P(None, TP, KV),
            P(),
            P(TP, KV),
            P(),
            P(TP, KV),
            P(TP, KV),
        ),
        out_specs=P(None, KV_TP),
        check_vma=False,
    )
```

```python
import functools

import jax
import jax.numpy as jnp
import numpy as np
from jax import lax
from jax.experimental import pallas as pl
from jax.experimental.pallas import tpu as pltpu
from jax.sharding import Mesh
from jax.sharding import PartitionSpec as P

HD = 64
KV = ("kv_0", "kv_1")
TP = ("z", "core")
KV_TP = (*KV, *TP)
LANES = 128

COST = 1 << 34
EPSILON = 1e-06
NEG_FILL = -1e30
F32 = jnp.float32
BF16 = jnp.bfloat16


def far_first(sizes):
    order = np.arange(np.prod(sizes)).reshape(sizes)
    for dim, size in enumerate(sizes):
        if size > 2:
            order = np.roll(order, -(size // 2), axis=dim)
    return [[int(index) for index in order.reshape(-1)]]


def exchange(copies, axes):
    sizes = [lax.axis_size(axis) for axis in ((axes,) if isinstance(axes, str) else axes)]
    return lax.all_to_all(
        copies, axes, split_axis=0, concat_axis=0, tiled=True, axis_index_groups=far_first(sizes)
    )


def near(array):
    return pltpu.with_memory_space_constraint(array, pltpu.VMEM)


def call(body, outs, name, scratch=()):
    return pl.pallas_call(
        body,
        out_shape=[jax.ShapeDtypeStruct(shape, dtype) for shape, dtype in outs],
        scratch_shapes=list(scratch),
        name=name,
        cost_estimate=pl.CostEstimate(flops=COST, bytes_accessed=COST // 256, transcendentals=0),
        compiler_params=pltpu.CompilerParams(vmem_limit_bytes=24 << 20),
    )


def rows_dot(left, right):
    return lax.dot_general(left, right, (((1,), (1,)), ((), ())), preferred_element_type=F32)


def iota(shape, dim):
    return lax.broadcasted_iota(jnp.int32, shape, dim)


def block_gain(gain_ref, block):
    gains = gain_ref[...].astype(F32)
    rows = iota(gains.shape, 0)
    first = jnp.sum(jnp.where(rows == 2 * block, gains, 0.0), axis=0, keepdims=True)
    second = jnp.sum(jnp.where(rows == 2 * block + 1, gains, 0.0), axis=0, keepdims=True)
    return jnp.concatenate([first, second], axis=1)


def spread_body(tokens, out):
    rows = tokens[...].astype(F32)
    line = jnp.concatenate([rows[at : at + 1] for at in range(rows.shape[0])], axis=1)
    out[...] = jnp.broadcast_to(line[None], out.shape)


def project_body(got, gain, query_w, key_w, value_w, forget_w, first_out, parts_out, block_out):
    position = lax.axis_index("kv_0") * 4 + lax.axis_index("kv_1")
    head = lax.axis_index("z") * 2 + lax.axis_index("core")
    peers = got.shape[0]
    sequences = block_out.shape[0]
    columns = LANES // sequences
    lines = jnp.concatenate([got[peers // 2 :], got[: peers // 2]], axis=0)
    spread = jnp.broadcast_to(lines, (peers, columns, LANES)).reshape(peers * columns, LANES)
    keep = (iota(spread.shape, 1) // sequences) == (iota(spread.shape, 0) % columns)
    fold = (iota((sequences, LANES), 1) % sequences) == iota((sequences, LANES), 0)
    block = rows_dot(
        jnp.where(fold, 1.0, 0.0).astype(BF16), jnp.where(keep, spread, 0.0).astype(BF16)
    )
    block_out[...] = block
    own = (block * block_gain(gain, position)).astype(BF16)
    query = rows_dot(own, query_w[...])
    key = rows_dot(own, key_w[...])
    value = rows_dot(own, value_w[...])
    width = block.shape[1]
    gate_rows = forget_w[:, pl.ds(pl.multiple_of(position * width, width), width)]
    gates = rows_dot(own, gate_rows)
    gate = jnp.sum(jnp.where(iota(gates.shape, 1) == head, gates, 0.0), axis=1, keepdims=True)
    squares = jnp.sum(block * block, axis=1, keepdims=True)
    lane = iota((sequences, LANES - HD), 1)
    rest = jnp.where(lane == 0, gate, jnp.where(lane == 1, squares, 0.0))
    line = jnp.concatenate([query, rest], axis=1)
    first_out[...] = jnp.broadcast_to(line[None], first_out.shape)
    parts_out[...] = jnp.concatenate([key, value], axis=1)


def pieces(column):
    high = column.astype(BF16).astype(F32)
    middle = (column - high).astype(BF16).astype(F32)
    return high, middle, column - high - middle


def attend_body(model_width, got, parts, pairs, gates, lengths, second_out, row_out):
    position = lax.axis_index("kv_0") * 4 + lax.axis_index("kv_1")
    sequences = parts.shape[0]
    count = gates.shape[2]
    line = jnp.sum(got[...], axis=0)
    scale = lax.rsqrt(line[:, HD + 1 : HD + 2] / model_width + EPSILON)
    query = (line[:, :HD] * scale).astype(BF16)
    forget = jax.nn.log_sigmoid(line[:, HD : HD + 1] * scale)
    wide = sequences * HD
    own_group = (iota((sequences, wide), 1) // HD) == iota((sequences, wide), 0)
    spread = jnp.concatenate([query.astype(F32)] * sequences, axis=1)
    spread = jnp.where(own_group, spread, 0.0).astype(BF16)
    keys = pairs[:, 0, 0].reshape(wide, count)
    raw = jnp.dot(spread, keys, preferred_element_type=F32)
    diagonal = iota((sequences, sequences), 0) == iota((sequences, sequences), 1)
    ends = jnp.broadcast_to(lengths[...].reshape(1, sequences), (sequences, sequences))
    ends = jnp.sum(jnp.where(diagonal, ends, 0), axis=1, keepdims=True) - position * count
    live = iota((sequences, count), 1) < ends
    scores = jnp.where(live, raw * HD ** (-0.5) + gates[:, 0, :], NEG_FILL)
    top = jnp.max(scores, axis=1, keepdims=True)
    weights = jnp.where(live, jnp.exp(scores - top), 0.0)
    total = jnp.sum(weights, axis=1, keepdims=True)
    values = pairs[:, 0, 1].reshape(wide, count)
    sums = jnp.where(own_group, rows_dot(weights.astype(BF16), values), 0.0)
    folded = sums[:, :LANES]
    for at in range(LANES, wide, LANES):
        folded = folded + sums[:, at : at + LANES]
    block_sum = folded[:, :HD] + folded[:, HD:]
    own = jnp.sum(query.astype(F32) * parts[:, :HD], axis=1, keepdims=True)
    lane = iota((sequences, LANES), 1)
    stats = jnp.zeros((sequences, LANES), F32)
    for at, piece in enumerate((*pieces(top), *pieces(total), *pieces(own))):
        stats = jnp.where(lane == at, piece, stats)
    out = jnp.concatenate([block_sum, parts[:, HD:], stats], axis=1).astype(BF16)
    second_out[...] = jnp.broadcast_to(out[None], second_out.shape)
    row_out[...] = jnp.where(lane == 0, forget, jnp.where(lane == 1, scale, 0.0))


def combine_body(got, row, output_w, out):
    sums = got[:, :, :HD].astype(F32)
    value_parts = got[:, :, HD:LANES].astype(F32)
    stats = got[:, :, LANES:].astype(F32)
    forget, scale = row[:, 0:1], row[:, 1:2]

    def stat(at):
        return stats[:, :, at : at + 1] + stats[:, :, at + 1 : at + 2] + stats[:, :, at + 2 : at + 3]

    tops = stat(0) + forget[None]
    own_score = jnp.sum(stat(6), axis=0) * scale * HD ** (-0.5)
    value_new = (jnp.sum(value_parts, axis=0) * scale).astype(BF16).astype(F32)
    highest = jnp.maximum(jnp.max(tops, axis=0), own_score)
    factors = jnp.exp(tops - highest[None])
    own_factor = jnp.exp(own_score - highest)
    numerator = jnp.sum(factors * sums, axis=0) + own_factor * value_new
    denominator = jnp.sum(factors * stat(3), axis=0) + own_factor
    attended = (numerator / denominator).astype(BF16)
    projected = jnp.dot(attended, output_w[...], preferred_element_type=F32)
    out[...] = jnp.broadcast_to(projected[None], out.shape)


def mix_body(got, block, gain, up_w, third_out, middle_out):
    position = lax.axis_index("kv_0") * 4 + lax.axis_index("kv_1")
    projected = jnp.sum(got[...].astype(F32), axis=0)
    middle = (block[...] + projected).astype(BF16)
    middle_out[...] = middle
    wide = middle.astype(F32)
    scaled = (wide * block_gain(gain, position)).astype(BF16)
    hidden = rows_dot(scaled, up_w[...])
    squares = jnp.sum(wide * wide, axis=1, keepdims=True)
    lane = iota((wide.shape[0], LANES), 1)
    stats = jnp.zeros(lane.shape, F32)
    for at, piece in enumerate(pieces(squares)):
        stats = jnp.where(lane == at, piece, stats)
    out = jnp.concatenate([hidden, stats], axis=1).astype(BF16)
    third_out[...] = jnp.broadcast_to(out[None], third_out.shape)


def down_body(model_width, got, down_w, out, turned):
    summed = jnp.sum(got[...].astype(F32), axis=0)
    units = down_w.shape[0]
    squares = summed[:, units : units + 1] + summed[:, units + 1 : units + 2]
    squares = squares + summed[:, units + 2 : units + 3]
    scale = lax.rsqrt(squares / model_width + EPSILON)
    activated = jnp.square(jax.nn.relu(summed[:, :units] * scale)).astype(BF16)
    sequences = activated.shape[0]
    down = jnp.dot(activated, down_w[...], preferred_element_type=F32)
    turned[...] = down.T
    peers = out.shape[0]
    columns = LANES // sequences
    lines = [turned[pl.ds(at, peers, stride=columns), :] for at in range(columns)]
    lines = jnp.concatenate(lines, axis=1)
    lines = jnp.concatenate([lines[peers // 2 :], lines[: peers // 2]], axis=0)
    out[...] = lines.reshape(out.shape)


def finish_body(got, middle, out):
    head = lax.axis_index("z") * 2 + lax.axis_index("core")
    columns, sequences = out.shape
    line = jnp.sum(got[...], axis=0)
    own_shape = (columns, middle.shape[1])
    chosen = iota(own_shape, 1) == iota(own_shape, 0) + head * columns
    own = rows_dot(jnp.where(chosen, 1.0, 0.0).astype(BF16), middle[...])
    down = jnp.concatenate(
        [line[:, at * sequences : (at + 1) * sequences] for at in range(columns)], axis=0
    )
    out[...] = (own + down).astype(BF16)


def local(
    tokens,
    attention_gain,
    query_weight,
    key_weight,
    value_weight,
    forget_weight,
    cached_pairs,
    cached_gates,
    lengths,
    output_weight,
    mixer_gain,
    up_weight,
    down_weight,
):
    sequences, own_columns = tokens.shape
    blocks, heads = lax.axis_size(KV), lax.axis_size(TP)
    width = query_weight.shape[1]
    model_width = width * blocks
    hidden_units = up_weight.shape[0]

    (line,) = call(spread_body, [((heads, 1, sequences * own_columns), F32)], "spread")(tokens.T)
    got = exchange(line, TP)
    first, parts, block = call(
        project_body,
        [((blocks, sequences, LANES), F32), ((sequences, LANES), F32), ((sequences, width), F32)],
        "project",
    )(
        got,
        near(attention_gain.reshape(-1, LANES)),
        near(query_weight),
        near(key_weight),
        near(value_weight),
        near(forget_weight),
    )
    got = exchange(first, KV)
    second, row = call(
        functools.partial(attend_body, model_width),
        [((blocks, sequences, 2 * LANES), BF16), ((sequences, LANES), F32)],
        "attend",
    )(got, parts, near(cached_pairs), near(cached_gates), near(lengths))
    got = exchange(second, KV)
    (projected,) = call(combine_body, [((2, sequences, width), F32)], "combine")(
        got, row, near(output_weight)
    )
    projected = jnp.sum(exchange(projected, "core"), axis=0).astype(BF16)
    got = exchange(jnp.broadcast_to(projected, (lax.axis_size("z"), *projected.shape)), "z")
    third, middle = call(
        mix_body,
        [((blocks, sequences, hidden_units + LANES), BF16), ((sequences, width), BF16)],
        "mix",
    )(got, block, near(mixer_gain.reshape(-1, LANES)), near(up_weight))
    got = exchange(third, KV)
    (down,) = call(
        functools.partial(down_body, model_width),
        [((heads, 1, LANES), F32)],
        "down",
        [pltpu.VMEM((width, sequences), F32)],
    )(got, near(down_weight))
    got = exchange(down, TP)
    (out,) = call(finish_body, [((own_columns, sequences), BF16)], "finish")(got, middle)
    return out.T


def solution(mesh):
    split = Mesh(mesh.devices.reshape(4, 4, 16, 2), KV_TP)
    return jax.shard_map(
        local,
        mesh=split,
        in_specs=(
            P(None, KV_TP),
            P(),
            P(TP, KV),
            P(TP, KV),
            P(TP, KV),
            P(),
            P(None, TP, None, None, KV),
            P(None, TP, KV),
            P(),
            P(TP, KV),
            P(),
            P(TP, KV),
            P(TP, KV),
        ),
        out_specs=P(None, KV_TP),
        check_vma=False,
    )
```

```python
import functools

import jax
import jax.numpy as jnp
import numpy as np
from jax import lax
from jax.experimental import pallas as pl
from jax.experimental.pallas import tpu as pltpu
from jax.sharding import Mesh
from jax.sharding import PartitionSpec as P

HD = 64
KV = ("kv_0", "kv_1")
TP = ("z", "core")
KV_TP = (*KV, *TP)
LANES = 128

COST = 1 << 34
EPSILON = 1e-06
NEG_FILL = -1e30
F32 = jnp.float32
BF16 = jnp.bfloat16


FIRST_Z, FIRST_TP = 9, 19


def group_of(axes):
    if axes == KV:
        order = np.roll(np.arange(16).reshape(4, 4), (-2, -2), (0, 1))
    elif axes == TP:
        order = np.roll(np.arange(32), -FIRST_TP)
    else:
        order = np.roll(np.arange(16), -FIRST_Z)
    return [[int(index) for index in order.reshape(-1)]]


def exchange(copies, axes):
    return lax.all_to_all(
        copies, axes, split_axis=0, concat_axis=0, tiled=True, axis_index_groups=group_of(axes)
    )


def near(array):
    return pltpu.with_memory_space_constraint(array, pltpu.VMEM)


def call(body, outs, name, scratch=()):
    return pl.pallas_call(
        body,
        out_shape=[jax.ShapeDtypeStruct(shape, dtype) for shape, dtype in outs],
        scratch_shapes=list(scratch),
        name=name,
        cost_estimate=pl.CostEstimate(flops=COST, bytes_accessed=COST // 256, transcendentals=0),
        compiler_params=pltpu.CompilerParams(vmem_limit_bytes=24 << 20),
    )


def rows_dot(left, right):
    return lax.dot_general(left, right, (((1,), (1,)), ((), ())), preferred_element_type=F32)


def iota(shape, dim):
    return lax.broadcasted_iota(jnp.int32, shape, dim)


def block_gain(gain_ref, block):
    gains = gain_ref[...].astype(F32)
    rows = iota(gains.shape, 0)
    first = jnp.sum(jnp.where(rows == 2 * block, gains, 0.0), axis=0, keepdims=True)
    second = jnp.sum(jnp.where(rows == 2 * block + 1, gains, 0.0), axis=0, keepdims=True)
    return jnp.concatenate([first, second], axis=1)


def spread_body(tokens, out):
    rows = tokens[...].astype(F32)
    line = jnp.concatenate([rows[at : at + 1] for at in range(rows.shape[0])], axis=1)
    out[...] = jnp.broadcast_to(line[None], out.shape)


def project_body(got, gain, query_w, key_w, value_w, forget_w, first_out, parts_out, block_out):
    position = lax.axis_index("kv_0") * 4 + lax.axis_index("kv_1")
    head = lax.axis_index("z") * 2 + lax.axis_index("core")
    peers = got.shape[0]
    sequences = block_out.shape[0]
    columns = LANES // sequences
    lines = jnp.concatenate([got[peers - FIRST_TP :], got[: peers - FIRST_TP]], axis=0)
    spread = jnp.broadcast_to(lines, (peers, columns, LANES)).reshape(peers * columns, LANES)
    keep = (iota(spread.shape, 1) // sequences) == (iota(spread.shape, 0) % columns)
    fold = (iota((sequences, LANES), 1) % sequences) == iota((sequences, LANES), 0)
    block = rows_dot(
        jnp.where(fold, 1.0, 0.0).astype(BF16), jnp.where(keep, spread, 0.0).astype(BF16)
    )
    block_out[...] = block
    own = (block * block_gain(gain, position)).astype(BF16)
    query = rows_dot(own, query_w[...])
    key = rows_dot(own, key_w[...])
    value = rows_dot(own, value_w[...])
    width = block.shape[1]
    gate_rows = forget_w[:, pl.ds(pl.multiple_of(position * width, width), width)]
    gates = rows_dot(own, gate_rows)
    gate = jnp.sum(jnp.where(iota(gates.shape, 1) == head, gates, 0.0), axis=1, keepdims=True)
    squares = jnp.sum(block * block, axis=1, keepdims=True)
    lane = iota((sequences, LANES - HD), 1)
    rest = jnp.where(lane == 0, gate, jnp.where(lane == 1, squares, 0.0))
    line = jnp.concatenate([query, rest], axis=1)
    first_out[...] = jnp.broadcast_to(line[None], first_out.shape)
    parts_out[...] = jnp.concatenate([key, value], axis=1)


def pieces(column):
    high = column.astype(BF16).astype(F32)
    middle = (column - high).astype(BF16).astype(F32)
    return high, middle, column - high - middle


def attend_body(model_width, got, parts, pairs, gates, lengths, second_out, row_out):
    position = lax.axis_index("kv_0") * 4 + lax.axis_index("kv_1")
    sequences = parts.shape[0]
    count = gates.shape[2]
    line = jnp.sum(got[...], axis=0)
    scale = lax.rsqrt(line[:, HD + 1 : HD + 2] / model_width + EPSILON)
    query = (line[:, :HD] * scale).astype(BF16)
    forget = jax.nn.log_sigmoid(line[:, HD : HD + 1] * scale)
    wide = sequences * HD
    own_group = (iota((sequences, wide), 1) // HD) == iota((sequences, wide), 0)
    spread = jnp.concatenate([query.astype(F32)] * sequences, axis=1)
    spread = jnp.where(own_group, spread, 0.0).astype(BF16)
    keys = pairs[:, 0, 0].reshape(wide, count)
    raw = jnp.dot(spread, keys, preferred_element_type=F32)
    diagonal = iota((sequences, sequences), 0) == iota((sequences, sequences), 1)
    ends = jnp.broadcast_to(lengths[...].reshape(1, sequences), (sequences, sequences))
    ends = jnp.sum(jnp.where(diagonal, ends, 0), axis=1, keepdims=True) - position * count
    live = iota((sequences, count), 1) < ends
    scores = jnp.where(live, raw * HD ** (-0.5) + gates[:, 0, :], NEG_FILL)
    top = jnp.max(scores, axis=1, keepdims=True)
    weights = jnp.where(live, jnp.exp(scores - top), 0.0)
    total = jnp.sum(weights, axis=1, keepdims=True)
    values = pairs[:, 0, 1].reshape(wide, count)
    sums = jnp.where(own_group, rows_dot(weights.astype(BF16), values), 0.0)
    folded = sums[:, :LANES]
    for at in range(LANES, wide, LANES):
        folded = folded + sums[:, at : at + LANES]
    block_sum = folded[:, :HD] + folded[:, HD:]
    own = jnp.sum(query.astype(F32) * parts[:, :HD], axis=1, keepdims=True)
    lane = iota((sequences, LANES), 1)
    stats = jnp.zeros((sequences, LANES), F32)
    for at, piece in enumerate((*pieces(top), *pieces(total), *pieces(own))):
        stats = jnp.where(lane == at, piece, stats)
    out = jnp.concatenate([block_sum, parts[:, HD:], stats], axis=1).astype(BF16)
    second_out[...] = jnp.broadcast_to(out[None], second_out.shape)
    row_out[...] = jnp.where(lane == 0, forget, jnp.where(lane == 1, scale, 0.0))


def combine_body(got, row, output_w, out):
    sums = got[:, :, :HD].astype(F32)
    value_parts = got[:, :, HD:LANES].astype(F32)
    stats = got[:, :, LANES:].astype(F32)
    forget, scale = row[:, 0:1], row[:, 1:2]

    def stat(at):
        return stats[:, :, at : at + 1] + stats[:, :, at + 1 : at + 2] + stats[:, :, at + 2 : at + 3]

    tops = stat(0) + forget[None]
    own_score = jnp.sum(stat(6), axis=0) * scale * HD ** (-0.5)
    value_new = (jnp.sum(value_parts, axis=0) * scale).astype(BF16).astype(F32)
    highest = jnp.maximum(jnp.max(tops, axis=0), own_score)
    factors = jnp.exp(tops - highest[None])
    own_factor = jnp.exp(own_score - highest)
    numerator = jnp.sum(factors * sums, axis=0) + own_factor * value_new
    denominator = jnp.sum(factors * stat(3), axis=0) + own_factor
    attended = (numerator / denominator).astype(BF16)
    projected = jnp.dot(attended, output_w[...], preferred_element_type=F32)
    out[...] = projected


def mix_body(got, block, gain, up_w, third_out, middle_out):
    position = lax.axis_index("kv_0") * 4 + lax.axis_index("kv_1")
    projected = jnp.sum(got[...].astype(F32), axis=0)
    middle = (block[...] + projected).astype(BF16)
    middle_out[...] = middle
    wide = middle.astype(F32)
    scaled = (wide * block_gain(gain, position)).astype(BF16)
    hidden = rows_dot(scaled, up_w[...])
    squares = jnp.sum(wide * wide, axis=1, keepdims=True)
    sequences, units = hidden.shape
    diagonal = iota((sequences, LANES), 0) == iota((sequences, LANES), 1)
    across = jnp.sum(jnp.where(diagonal, squares, 0.0), axis=0, keepdims=True)
    row = iota((8, LANES), 0)
    stats = jnp.zeros(row.shape, F32)
    for at, piece in enumerate(pieces(across)):
        stats = jnp.where(row == at, piece, stats)
    parts = [hidden[:, at : at + LANES] for at in range(0, units, LANES)]
    out = jnp.concatenate([*parts, stats], axis=0).astype(BF16)
    third_out[...] = jnp.broadcast_to(out[None], third_out.shape)


def down_body(model_width, got, down_w, out, turned):
    summed = jnp.sum(got[...].astype(F32), axis=0)
    sequences = turned.shape[1]
    units = down_w.shape[0] // LANES * sequences
    parts = [summed[at : at + sequences] for at in range(0, units, sequences)]
    across = jnp.sum(summed[units : units + 3], axis=0, keepdims=True)
    diagonal = iota((sequences, LANES), 0) == iota((sequences, LANES), 1)
    squares = jnp.sum(jnp.where(diagonal, across, 0.0), axis=1, keepdims=True)
    scale = lax.rsqrt(squares / model_width + EPSILON)
    activated = [jnp.square(jax.nn.relu(part * scale)).astype(BF16) for part in parts]
    activated = jnp.concatenate(activated, axis=1)
    down = jnp.dot(activated, down_w[...], preferred_element_type=F32)
    turned[...] = down.T
    peers = out.shape[0]
    columns = LANES // sequences
    lines = [turned[pl.ds(at, peers, stride=columns), :] for at in range(columns)]
    lines = jnp.concatenate(lines, axis=1).reshape(out.shape)
    out[...] = jnp.concatenate([lines[FIRST_TP:], lines[:FIRST_TP]], axis=0)


def finish_body(got, middle, out):
    head = lax.axis_index("z") * 2 + lax.axis_index("core")
    columns, sequences = out.shape
    line = jnp.sum(got[...], axis=0)
    own_shape = (columns, middle.shape[1])
    chosen = iota(own_shape, 1) == iota(own_shape, 0) + head * columns
    own = rows_dot(jnp.where(chosen, 1.0, 0.0).astype(BF16), middle[...])
    down = jnp.concatenate(
        [line[:, at * sequences : (at + 1) * sequences] for at in range(columns)], axis=0
    )
    out[...] = (own + down).astype(BF16)


def local(
    tokens,
    attention_gain,
    query_weight,
    key_weight,
    value_weight,
    forget_weight,
    cached_pairs,
    cached_gates,
    lengths,
    output_weight,
    mixer_gain,
    up_weight,
    down_weight,
):
    sequences, own_columns = tokens.shape
    blocks, heads = lax.axis_size(KV), lax.axis_size(TP)
    width = query_weight.shape[1]
    model_width = width * blocks
    hidden_units = up_weight.shape[0]

    (line,) = call(spread_body, [((heads, 1, sequences * own_columns), F32)], "spread")(tokens.T)
    got = exchange(line, TP)
    first, parts, block = call(
        project_body,
        [((blocks, sequences, LANES), F32), ((sequences, LANES), F32), ((sequences, width), F32)],
        "project",
    )(
        got,
        near(attention_gain.reshape(-1, LANES)),
        near(query_weight),
        near(key_weight),
        near(value_weight),
        near(forget_weight),
    )
    got = exchange(first, KV)
    second, row = call(
        functools.partial(attend_body, model_width),
        [((blocks, sequences, 2 * LANES), BF16), ((sequences, LANES), F32)],
        "attend",
    )(got, parts, near(cached_pairs), near(cached_gates), near(lengths))
    got = exchange(second, KV)
    (projected,) = call(combine_body, [((sequences, width), F32)], "combine")(
        got, row, near(output_weight)
    )
    projected = projected + lax.ppermute(projected, "core", [(0, 1), (1, 0)])
    projected = projected.astype(BF16)
    got = exchange(jnp.broadcast_to(projected, (lax.axis_size("z"), *projected.shape)), "z")
    third, middle = call(
        mix_body,
        [((blocks, sequences * hidden_units // LANES + 8, LANES), BF16), ((sequences, width), BF16)],
        "mix",
    )(got, block, near(mixer_gain.reshape(-1, LANES)), near(up_weight))
    got = exchange(third, KV)
    (down,) = call(
        functools.partial(down_body, model_width),
        [((heads, 1, LANES), F32)],
        "down",
        [pltpu.VMEM((width, sequences), F32)],
    )(got, near(down_weight))
    got = exchange(down, TP)
    (out,) = call(finish_body, [((own_columns, sequences), BF16)], "finish")(got, middle)
    return out.T


def solution(mesh):
    split = Mesh(mesh.devices.reshape(4, 4, 16, 2), KV_TP)
    return jax.shard_map(
        local,
        mesh=split,
        in_specs=(
            P(None, KV_TP),
            P(),
            P(TP, KV),
            P(TP, KV),
            P(TP, KV),
            P(),
            P(None, TP, None, None, KV),
            P(None, TP, KV),
            P(),
            P(TP, KV),
            P(),
            P(TP, KV),
            P(TP, KV),
        ),
        out_specs=P(None, KV_TP),
        check_vma=False,
    )
```

```python
import functools

import jax
import jax.numpy as jnp
import numpy as np
from jax import lax
from jax.experimental import pallas as pl
from jax.experimental.pallas import tpu as pltpu
from jax.sharding import Mesh
from jax.sharding import PartitionSpec as P

HD = 64
KV = ("kv_0", "kv_1")
TP = ("z", "core")
KV_TP = (*KV, *TP)
LANES = 128

COST = 1 << 34
EPSILON = 1e-06
NEG_FILL = -1e30
F32 = jnp.float32
BF16 = jnp.bfloat16


FIRST_Z, FIRST_TP = 9, 19


def group_of(axes):
    if axes == KV:
        row, column = np.divmod(np.arange(16), 4)
        order = (row + 2 * column + 2) % 4 * 4 + (column + 2) % 4
    elif axes == TP:
        order = np.roll(np.arange(32), -FIRST_TP)
    else:
        order = (FIRST_Z + 7 * np.arange(16)) % 16
    return [[int(index) for index in order.reshape(-1)]]


def exchange(copies, axes):
    return lax.all_to_all(
        copies, axes, split_axis=0, concat_axis=0, tiled=True, axis_index_groups=group_of(axes)
    )


def near(array):
    return pltpu.with_memory_space_constraint(array, pltpu.VMEM)


def call(body, outs, name, scratch=()):
    return pl.pallas_call(
        body,
        out_shape=[jax.ShapeDtypeStruct(shape, dtype) for shape, dtype in outs],
        scratch_shapes=list(scratch),
        name=name,
        cost_estimate=pl.CostEstimate(flops=COST, bytes_accessed=COST // 256, transcendentals=0),
        compiler_params=pltpu.CompilerParams(vmem_limit_bytes=24 << 20),
    )


def rows_dot(left, right):
    return lax.dot_general(left, right, (((1,), (1,)), ((), ())), preferred_element_type=F32)


def iota(shape, dim):
    return lax.broadcasted_iota(jnp.int32, shape, dim)


def block_gain(gain_ref, block):
    gains = gain_ref[...].astype(F32)
    rows = iota(gains.shape, 0)
    first = jnp.sum(jnp.where(rows == 2 * block, gains, 0.0), axis=0, keepdims=True)
    second = jnp.sum(jnp.where(rows == 2 * block + 1, gains, 0.0), axis=0, keepdims=True)
    return jnp.concatenate([first, second], axis=1)


def spread_body(tokens, out):
    rows = tokens[...].astype(F32)
    line = jnp.concatenate([rows[at : at + 1] for at in range(rows.shape[0])], axis=1)
    out[...] = jnp.broadcast_to(line[None], out.shape)


def project_body(got, gain, query_w, key_w, value_w, forget_w, first_out, parts_out, block_out):
    position = lax.axis_index("kv_0") * 4 + lax.axis_index("kv_1")
    head = lax.axis_index("z") * 2 + lax.axis_index("core")
    peers = got.shape[0]
    sequences = block_out.shape[0]
    columns = LANES // sequences
    lines = jnp.concatenate([got[peers - FIRST_TP :], got[: peers - FIRST_TP]], axis=0)
    spread = jnp.broadcast_to(lines, (peers, columns, LANES)).reshape(peers * columns, LANES)
    keep = (iota(spread.shape, 1) // sequences) == (iota(spread.shape, 0) % columns)
    fold = (iota((sequences, LANES), 1) % sequences) == iota((sequences, LANES), 0)
    block = rows_dot(
        jnp.where(fold, 1.0, 0.0).astype(BF16), jnp.where(keep, spread, 0.0).astype(BF16)
    )
    block_out[...] = block
    own = (block * block_gain(gain, position)).astype(BF16)
    query = rows_dot(own, query_w[...])
    key = rows_dot(own, key_w[...])
    value = rows_dot(own, value_w[...])
    width = block.shape[1]
    gate_rows = forget_w[:, pl.ds(pl.multiple_of(position * width, width), width)]
    gates = rows_dot(own, gate_rows)
    gate = jnp.sum(jnp.where(iota(gates.shape, 1) == head, gates, 0.0), axis=1, keepdims=True)
    squares = jnp.sum(block * block, axis=1, keepdims=True)
    lane = iota((sequences, LANES - HD), 1)
    rest = jnp.where(lane == 0, gate, jnp.where(lane == 1, squares, 0.0))
    line = jnp.concatenate([query, rest], axis=1)
    first_out[...] = jnp.broadcast_to(line[None], first_out.shape)
    parts_out[...] = jnp.concatenate([key, value], axis=1)


def pieces(column):
    high = column.astype(BF16).astype(F32)
    middle = (column - high).astype(BF16).astype(F32)
    return high, middle, column - high - middle


def attend_body(model_width, got, parts, pairs, gates, lengths, second_out, row_out):
    position = lax.axis_index("kv_0") * 4 + lax.axis_index("kv_1")
    sequences = parts.shape[0]
    count = gates.shape[2]
    line = jnp.sum(got[...], axis=0)
    scale = lax.rsqrt(line[:, HD + 1 : HD + 2] / model_width + EPSILON)
    query = (line[:, :HD] * scale).astype(BF16)
    forget = jax.nn.log_sigmoid(line[:, HD : HD + 1] * scale)
    wide = sequences * HD
    own_group = (iota((sequences, wide), 1) // HD) == iota((sequences, wide), 0)
    spread = jnp.concatenate([query.astype(F32)] * sequences, axis=1)
    spread = jnp.where(own_group, spread, 0.0).astype(BF16)
    keys = pairs[:, 0, 0].reshape(wide, count)
    raw = jnp.dot(spread, keys, preferred_element_type=F32)
    diagonal = iota((sequences, sequences), 0) == iota((sequences, sequences), 1)
    ends = jnp.broadcast_to(lengths[...].reshape(1, sequences), (sequences, sequences))
    ends = jnp.sum(jnp.where(diagonal, ends, 0), axis=1, keepdims=True) - position * count
    live = iota((sequences, count), 1) < ends
    scores = jnp.where(live, raw * HD ** (-0.5) + gates[:, 0, :], NEG_FILL)
    top = jnp.max(scores, axis=1, keepdims=True)
    weights = jnp.where(live, jnp.exp(scores - top), 0.0)
    total = jnp.sum(weights, axis=1, keepdims=True)
    values = pairs[:, 0, 1].reshape(wide, count)
    sums = jnp.where(own_group, rows_dot(weights.astype(BF16), values), 0.0)
    folded = sums[:, :LANES]
    for at in range(LANES, wide, LANES):
        folded = folded + sums[:, at : at + LANES]
    block_sum = folded[:, :HD] + folded[:, HD:]
    own = jnp.sum(query.astype(F32) * parts[:, :HD], axis=1, keepdims=True)
    lane = iota((sequences, LANES), 1)
    stats = jnp.zeros((sequences, LANES), F32)
    for at, piece in enumerate((*pieces(top), *pieces(total), *pieces(own))):
        stats = jnp.where(lane == at, piece, stats)
    out = jnp.concatenate([block_sum, parts[:, HD:], stats], axis=1).astype(BF16)
    second_out[...] = jnp.broadcast_to(out[None], second_out.shape)
    row_out[...] = jnp.where(lane == 0, forget, jnp.where(lane == 1, scale, 0.0))


def combine_body(got, row, output_w, out):
    sums = got[:, :, :HD].astype(F32)
    value_parts = got[:, :, HD:LANES].astype(F32)
    stats = got[:, :, LANES:].astype(F32)
    forget, scale = row[:, 0:1], row[:, 1:2]

    def stat(at):
        return stats[:, :, at : at + 1] + stats[:, :, at + 1 : at + 2] + stats[:, :, at + 2 : at + 3]

    tops = stat(0) + forget[None]
    own_score = jnp.sum(stat(6), axis=0) * scale * HD ** (-0.5)
    value_new = (jnp.sum(value_parts, axis=0) * scale).astype(BF16).astype(F32)
    highest = jnp.maximum(jnp.max(tops, axis=0), own_score)
    factors = jnp.exp(tops - highest[None])
    own_factor = jnp.exp(own_score - highest)
    numerator = jnp.sum(factors * sums, axis=0) + own_factor * value_new
    denominator = jnp.sum(factors * stat(3), axis=0) + own_factor
    attended = (numerator / denominator).astype(BF16)
    projected = jnp.dot(attended, output_w[...], preferred_element_type=F32)
    out[...] = projected


def mix_body(got, block, gain, up_w, third_out, middle_out):
    position = lax.axis_index("kv_0") * 4 + lax.axis_index("kv_1")
    projected = jnp.sum(got[...].astype(F32), axis=0)
    middle = (block[...] + projected).astype(BF16)
    middle_out[...] = middle
    wide = middle.astype(F32)
    scaled = (wide * block_gain(gain, position)).astype(BF16)
    hidden = rows_dot(scaled, up_w[...])
    squares = jnp.sum(wide * wide, axis=1, keepdims=True)
    sequences, units = hidden.shape
    diagonal = iota((sequences, LANES), 0) == iota((sequences, LANES), 1)
    across = jnp.sum(jnp.where(diagonal, squares, 0.0), axis=0, keepdims=True)
    row = iota((8, LANES), 0)
    stats = jnp.zeros(row.shape, F32)
    for at, piece in enumerate(pieces(across)):
        stats = jnp.where(row == at, piece, stats)
    parts = [hidden[:, at : at + LANES] for at in range(0, units, LANES)]
    out = jnp.concatenate([*parts, stats], axis=0).astype(BF16)
    third_out[...] = jnp.broadcast_to(out[None], third_out.shape)


def down_body(model_width, got, down_w, out, turned):
    summed = jnp.sum(got[...].astype(F32), axis=0)
    sequences = turned.shape[1]
    units = down_w.shape[0] // LANES * sequences
    parts = [summed[at : at + sequences] for at in range(0, units, sequences)]
    across = jnp.sum(summed[units : units + 3], axis=0, keepdims=True)
    diagonal = iota((sequences, LANES), 0) == iota((sequences, LANES), 1)
    squares = jnp.sum(jnp.where(diagonal, across, 0.0), axis=1, keepdims=True)
    scale = lax.rsqrt(squares / model_width + EPSILON)
    activated = [jnp.square(jax.nn.relu(part * scale)).astype(BF16) for part in parts]
    activated = jnp.concatenate(activated, axis=1)
    down = jnp.dot(activated, down_w[...], preferred_element_type=F32)
    turned[...] = down.T
    peers = out.shape[0]
    columns = LANES // sequences
    lines = [turned[pl.ds(at, peers, stride=columns), :] for at in range(columns)]
    lines = jnp.concatenate(lines, axis=1).reshape(out.shape)
    out[...] = jnp.concatenate([lines[FIRST_TP:], lines[:FIRST_TP]], axis=0)


def finish_body(got, middle, out):
    head = lax.axis_index("z") * 2 + lax.axis_index("core")
    columns, sequences = out.shape
    line = jnp.sum(got[...], axis=0)
    own_shape = (columns, middle.shape[1])
    chosen = iota(own_shape, 1) == iota(own_shape, 0) + head * columns
    own = rows_dot(jnp.where(chosen, 1.0, 0.0).astype(BF16), middle[...])
    down = jnp.concatenate(
        [line[:, at * sequences : (at + 1) * sequences] for at in range(columns)], axis=0
    )
    out[...] = (own + down).astype(BF16)


def local(
    tokens,
    attention_gain,
    query_weight,
    key_weight,
    value_weight,
    forget_weight,
    cached_pairs,
    cached_gates,
    lengths,
    output_weight,
    mixer_gain,
    up_weight,
    down_weight,
):
    sequences, own_columns = tokens.shape
    blocks, heads = lax.axis_size(KV), lax.axis_size(TP)
    width = query_weight.shape[1]
    model_width = width * blocks
    hidden_units = up_weight.shape[0]

    (line,) = call(spread_body, [((heads, 1, sequences * own_columns), F32)], "spread")(tokens.T)
    got = exchange(line, TP)
    first, parts, block = call(
        project_body,
        [((blocks, sequences, LANES), F32), ((sequences, LANES), F32), ((sequences, width), F32)],
        "project",
    )(
        got,
        near(attention_gain.reshape(-1, LANES)),
        near(query_weight),
        near(key_weight),
        near(value_weight),
        near(forget_weight),
    )
    got = exchange(first, KV)
    second, row = call(
        functools.partial(attend_body, model_width),
        [((blocks, sequences, 2 * LANES), BF16), ((sequences, LANES), F32)],
        "attend",
    )(got, parts, near(cached_pairs), near(cached_gates), near(lengths))
    got = exchange(second, KV)
    (projected,) = call(combine_body, [((sequences, width), F32)], "combine")(
        got, row, near(output_weight)
    )
    projected = projected + lax.ppermute(projected, "core", [(0, 1), (1, 0)])
    projected = projected.astype(BF16)
    got = exchange(jnp.broadcast_to(projected, (lax.axis_size("z"), *projected.shape)), "z")
    third, middle = call(
        mix_body,
        [((blocks, sequences * hidden_units // LANES + 8, LANES), BF16), ((sequences, width), BF16)],
        "mix",
    )(got, block, near(mixer_gain.reshape(-1, LANES)), near(up_weight))
    got = exchange(third, KV)
    (down,) = call(
        functools.partial(down_body, model_width),
        [((heads, 1, LANES), F32)],
        "down",
        [pltpu.VMEM((width, sequences), F32)],
    )(got, near(down_weight))
    got = exchange(down, TP)
    (out,) = call(finish_body, [((own_columns, sequences), BF16)], "finish")(got, middle)
    return out.T


def solution(mesh):
    split = Mesh(mesh.devices.reshape(4, 4, 16, 2), KV_TP)
    return jax.shard_map(
        local,
        mesh=split,
        in_specs=(
            P(None, KV_TP),
            P(),
            P(TP, KV),
            P(TP, KV),
            P(TP, KV),
            P(),
            P(None, TP, None, None, KV),
            P(None, TP, KV),
            P(),
            P(TP, KV),
            P(),
            P(TP, KV),
            P(TP, KV),
        ),
        out_specs=P(None, KV_TP),
        check_vma=False,
    )
```

```python
import functools

import jax
import jax.numpy as jnp
import numpy as np
from jax import lax
from jax.experimental import pallas as pl
from jax.experimental.pallas import tpu as pltpu
from jax.sharding import Mesh
from jax.sharding import PartitionSpec as P

HD = 64
KV = ("kv_0", "kv_1")
TP = ("z", "core")
KV_TP = (*KV, *TP)
LANES = 128

COST = 1 << 34
EPSILON = 1e-06
NEG_FILL = -1e30
F32 = jnp.float32
BF16 = jnp.bfloat16


FIRST_Z, FIRST_TP = 9, 19


def group_of(axes):
    if axes == KV:
        row, column = np.divmod(np.arange(16), 4)
        order = (row + 2 * column + 2) % 4 * 4 + (column + 2) % 4
    elif axes == TP:
        order = np.roll(np.arange(32), -FIRST_TP)
    else:
        order = (FIRST_Z + 7 * np.arange(16)) % 16
    return [[int(index) for index in order.reshape(-1)]]


def exchange(copies, axes):
    return lax.all_to_all(
        copies, axes, split_axis=0, concat_axis=0, tiled=True, axis_index_groups=group_of(axes)
    )


def near(array):
    return pltpu.with_memory_space_constraint(array, pltpu.VMEM)


def call(body, outs, name, scratch=()):
    return pl.pallas_call(
        body,
        out_shape=[jax.ShapeDtypeStruct(shape, dtype) for shape, dtype in outs],
        scratch_shapes=list(scratch),
        name=name,
        cost_estimate=pl.CostEstimate(flops=COST, bytes_accessed=COST // 256, transcendentals=0),
        compiler_params=pltpu.CompilerParams(vmem_limit_bytes=24 << 20),
    )


def rows_dot(left, right):
    return lax.dot_general(left, right, (((1,), (1,)), ((), ())), preferred_element_type=F32)


def iota(shape, dim):
    return lax.broadcasted_iota(jnp.int32, shape, dim)


def block_gain(gain_ref, block):
    gains = gain_ref[...].astype(F32)
    rows = iota(gains.shape, 0)
    first = jnp.sum(jnp.where(rows == 2 * block, gains, 0.0), axis=0, keepdims=True)
    second = jnp.sum(jnp.where(rows == 2 * block + 1, gains, 0.0), axis=0, keepdims=True)
    return jnp.concatenate([first, second], axis=1)


def spread_body(tokens, out):
    rows = tokens[...].astype(F32)
    line = jnp.concatenate([rows[at : at + 1] for at in range(rows.shape[0])], axis=1)
    out[...] = jnp.broadcast_to(line[None], out.shape)


def project_body(got, gain, query_w, key_w, value_w, forget_w, first_out, parts_out, block_out):
    position = lax.axis_index("kv_0") * 4 + lax.axis_index("kv_1")
    head = lax.axis_index("z") * 2 + lax.axis_index("core")
    peers = got.shape[0]
    sequences = block_out.shape[0]
    columns = LANES // sequences
    lines = jnp.concatenate([got[peers - FIRST_TP :], got[: peers - FIRST_TP]], axis=0)
    spread = jnp.broadcast_to(lines, (peers, columns, LANES)).reshape(peers * columns, LANES)
    keep = (iota(spread.shape, 1) // sequences) == (iota(spread.shape, 0) % columns)
    fold = (iota((sequences, LANES), 1) % sequences) == iota((sequences, LANES), 0)
    block = rows_dot(
        jnp.where(fold, 1.0, 0.0).astype(BF16), jnp.where(keep, spread, 0.0).astype(BF16)
    )
    block_out[...] = block
    own = (block * block_gain(gain, position)).astype(BF16)
    query = rows_dot(own, query_w[...])
    key = rows_dot(own, key_w[...])
    value = rows_dot(own, value_w[...])
    width = block.shape[1]
    gate_rows = forget_w[:, pl.ds(pl.multiple_of(position * width, width), width)]
    gates = rows_dot(own, gate_rows)
    gate = jnp.sum(jnp.where(iota(gates.shape, 1) == head, gates, 0.0), axis=1, keepdims=True)
    squares = jnp.sum(block * block, axis=1, keepdims=True)
    lane = iota((sequences, LANES - HD), 1)
    rest = jnp.where(lane == 0, gate, jnp.where(lane == 1, squares, 0.0))
    line = jnp.concatenate([query, rest], axis=1)
    first_out[...] = jnp.broadcast_to(line[None], first_out.shape)
    parts_out[...] = jnp.concatenate([key, value], axis=1)


def pieces(column):
    high = column.astype(BF16).astype(F32)
    middle = (column - high).astype(BF16).astype(F32)
    return high, middle, column - high - middle


def attend_body(model_width, got, parts, pairs, gates, lengths, second_out, row_out):
    position = lax.axis_index("kv_0") * 4 + lax.axis_index("kv_1")
    sequences = parts.shape[0]
    count = gates.shape[2]
    line = jnp.sum(got[...], axis=0)
    scale = lax.rsqrt(line[:, HD + 1 : HD + 2] / model_width + EPSILON)
    query = (line[:, :HD] * scale).astype(BF16)
    forget = jax.nn.log_sigmoid(line[:, HD : HD + 1] * scale)
    wide = sequences * HD
    own_group = (iota((sequences, wide), 1) // HD) == iota((sequences, wide), 0)
    spread = jnp.concatenate([query.astype(F32)] * sequences, axis=1)
    spread = jnp.where(own_group, spread, 0.0).astype(BF16)
    keys = pairs[:, 0, 0].reshape(wide, count)
    raw = jnp.dot(spread, keys, preferred_element_type=F32)
    diagonal = iota((sequences, sequences), 0) == iota((sequences, sequences), 1)
    ends = jnp.broadcast_to(lengths[...].reshape(1, sequences), (sequences, sequences))
    ends = jnp.sum(jnp.where(diagonal, ends, 0), axis=1, keepdims=True) - position * count
    live = iota((sequences, count), 1) < ends
    scores = jnp.where(live, raw * HD ** (-0.5) + gates[:, 0, :], NEG_FILL)
    top = jnp.max(scores, axis=1, keepdims=True)
    weights = jnp.where(live, jnp.exp(scores - top), 0.0)
    total = jnp.sum(weights, axis=1, keepdims=True)
    values = pairs[:, 0, 1].reshape(wide, count)
    sums = jnp.where(own_group, rows_dot(weights.astype(BF16), values), 0.0)
    folded = sums[:, :LANES]
    for at in range(LANES, wide, LANES):
        folded = folded + sums[:, at : at + LANES]
    block_sum = folded[:, :HD] + folded[:, HD:]
    own = jnp.sum(query.astype(F32) * parts[:, :HD], axis=1, keepdims=True)
    lane = iota((sequences, LANES), 1)
    stats = jnp.zeros((sequences, LANES), F32)
    for at, piece in enumerate((*pieces(top), *pieces(total), *pieces(own))):
        stats = jnp.where(lane == at, piece, stats)
    out = jnp.concatenate([block_sum, parts[:, HD:], stats], axis=1).astype(BF16)
    second_out[...] = jnp.broadcast_to(out[None], second_out.shape)
    row_out[...] = jnp.where(lane == 0, forget, jnp.where(lane == 1, scale, 0.0))


def combine_body(got, row, output_w, out):
    sums = got[:, :, :HD].astype(F32)
    value_parts = got[:, :, HD:LANES].astype(F32)
    stats = got[:, :, LANES:].astype(F32)
    forget, scale = row[:, 0:1], row[:, 1:2]

    def stat(at):
        return stats[:, :, at : at + 1] + stats[:, :, at + 1 : at + 2] + stats[:, :, at + 2 : at + 3]

    tops = stat(0) + forget[None]
    own_score = jnp.sum(stat(6), axis=0) * scale * HD ** (-0.5)
    value_new = (jnp.sum(value_parts, axis=0) * scale).astype(BF16).astype(F32)
    highest = jnp.maximum(jnp.max(tops, axis=0), own_score)
    factors = jnp.exp(tops - highest[None])
    own_factor = jnp.exp(own_score - highest)
    numerator = jnp.sum(factors * sums, axis=0) + own_factor * value_new
    denominator = jnp.sum(factors * stat(3), axis=0) + own_factor
    attended = (numerator / denominator).astype(BF16)
    projected = jnp.dot(attended, output_w[...], preferred_element_type=F32)
    out[...] = jnp.broadcast_to(projected.astype(BF16)[None], out.shape)


def mix_body(own, other, block, gain, up_w, third_out, middle_out):
    position = lax.axis_index("kv_0") * 4 + lax.axis_index("kv_1")
    middle = (block[...] + (own[...] + other[...])).astype(BF16)
    middle_out[...] = middle
    wide = middle.astype(F32)
    scaled = (wide * block_gain(gain, position)).astype(BF16)
    hidden = rows_dot(scaled, up_w[...])
    squares = jnp.sum(wide * wide, axis=1, keepdims=True)
    sequences, units = hidden.shape
    diagonal = iota((sequences, LANES), 0) == iota((sequences, LANES), 1)
    across = jnp.sum(jnp.where(diagonal, squares, 0.0), axis=0, keepdims=True)
    row = iota((8, LANES), 0)
    stats = jnp.zeros(row.shape, F32)
    for at, piece in enumerate(pieces(across)):
        stats = jnp.where(row == at, piece, stats)
    parts = [hidden[:, at : at + LANES] for at in range(0, units, LANES)]
    out = jnp.concatenate([*parts, stats], axis=0).astype(BF16)
    third_out[...] = jnp.broadcast_to(out[None], third_out.shape)


def down_body(model_width, got, down_w, out, turned):
    summed = jnp.sum(got[...].astype(F32), axis=0)
    sequences = turned.shape[1]
    units = down_w.shape[0] // LANES * sequences
    parts = [summed[at : at + sequences] for at in range(0, units, sequences)]
    across = jnp.sum(summed[units : units + 3], axis=0, keepdims=True)
    diagonal = iota((sequences, LANES), 0) == iota((sequences, LANES), 1)
    squares = jnp.sum(jnp.where(diagonal, across, 0.0), axis=1, keepdims=True)
    scale = lax.rsqrt(squares / model_width + EPSILON)
    activated = [jnp.square(jax.nn.relu(part * scale)).astype(BF16) for part in parts]
    activated = jnp.concatenate(activated, axis=1)
    down = jnp.dot(activated, down_w[...], preferred_element_type=F32)
    turned[...] = down.T
    peers = out.shape[0]
    columns = LANES // sequences
    lines = [turned[pl.ds(at, peers, stride=columns), :] for at in range(columns)]
    lines = jnp.concatenate(lines, axis=1).reshape(out.shape)
    out[...] = jnp.concatenate([lines[FIRST_TP:], lines[:FIRST_TP]], axis=0)


def finish_body(got, middle, out):
    head = lax.axis_index("z") * 2 + lax.axis_index("core")
    columns, sequences = out.shape
    line = jnp.sum(got[...], axis=0)
    own_shape = (columns, middle.shape[1])
    chosen = iota(own_shape, 1) == iota(own_shape, 0) + head * columns
    own = rows_dot(jnp.where(chosen, 1.0, 0.0).astype(BF16), middle[...])
    down = jnp.concatenate(
        [line[:, at * sequences : (at + 1) * sequences] for at in range(columns)], axis=0
    )
    out[...] = (own + down).astype(BF16)


def local(
    tokens,
    attention_gain,
    query_weight,
    key_weight,
    value_weight,
    forget_weight,
    cached_pairs,
    cached_gates,
    lengths,
    output_weight,
    mixer_gain,
    up_weight,
    down_weight,
):
    sequences, own_columns = tokens.shape
    blocks, heads = lax.axis_size(KV), lax.axis_size(TP)
    width = query_weight.shape[1]
    model_width = width * blocks
    hidden_units = up_weight.shape[0]

    (line,) = call(spread_body, [((heads, 1, sequences * own_columns), F32)], "spread")(tokens.T)
    got = exchange(line, TP)
    first, parts, block = call(
        project_body,
        [((blocks, sequences, LANES), F32), ((sequences, LANES), F32), ((sequences, width), F32)],
        "project",
    )(
        got,
        near(attention_gain.reshape(-1, LANES)),
        near(query_weight),
        near(key_weight),
        near(value_weight),
        near(forget_weight),
    )
    got = exchange(first, KV)
    second, row = call(
        functools.partial(attend_body, model_width),
        [((blocks, sequences, 2 * LANES), BF16), ((sequences, LANES), F32)],
        "attend",
    )(got, parts, near(cached_pairs), near(cached_gates), near(lengths))
    got = exchange(second, KV)
    (projected,) = call(
        combine_body, [((lax.axis_size("z"), sequences, width), BF16)], "combine"
    )(got, row, near(output_weight))
    own = jnp.sum(exchange(projected, "z").astype(F32), axis=0)
    other = lax.ppermute(own, "core", [(0, 1), (1, 0)])
    third, middle = call(
        mix_body,
        [((blocks, sequences * hidden_units // LANES + 8, LANES), BF16), ((sequences, width), BF16)],
        "mix",
    )(own, other, block, near(mixer_gain.reshape(-1, LANES)), near(up_weight))
    got = exchange(third, KV)
    (down,) = call(
        functools.partial(down_body, model_width),
        [((heads, 1, LANES), F32)],
        "down",
        [pltpu.VMEM((width, sequences), F32)],
    )(got, near(down_weight))
    got = exchange(down, TP)
    (out,) = call(finish_body, [((own_columns, sequences), BF16)], "finish")(got, middle)
    return out.T


def solution(mesh):
    split = Mesh(mesh.devices.reshape(4, 4, 16, 2), KV_TP)
    return jax.shard_map(
        local,
        mesh=split,
        in_specs=(
            P(None, KV_TP),
            P(),
            P(TP, KV),
            P(TP, KV),
            P(TP, KV),
            P(),
            P(None, TP, None, None, KV),
            P(None, TP, KV),
            P(),
            P(TP, KV),
            P(),
            P(TP, KV),
            P(TP, KV),
        ),
        out_specs=P(None, KV_TP),
        check_vma=False,
    )
```

```python
import functools

import jax
import jax.numpy as jnp
import numpy as np
from jax import lax
from jax.experimental import pallas as pl
from jax.experimental.pallas import tpu as pltpu
from jax.sharding import Mesh
from jax.sharding import PartitionSpec as P

HD = 64
KV = ("kv_0", "kv_1")
TP = ("z", "core")
KV_TP = (*KV, *TP)
LANES = 128

COST = 1 << 34
EPSILON = 1e-06
NEG_FILL = -1e30
F32 = jnp.float32
BF16 = jnp.bfloat16


FIRST_Z, FIRST_TP = 9, 19


def group_of(axes):
    if axes == KV:
        row, column = np.divmod(np.arange(16), 4)
        order = (row + 2 * column + 2) % 4 * 4 + (column + 2) % 4
    elif axes == TP:
        order = np.roll(np.arange(32), -FIRST_TP)
    else:
        order = (FIRST_Z + 7 * np.arange(16)) % 16
    return [[int(index) for index in order.reshape(-1)]]


def exchange(copies, axes):
    return lax.all_to_all(
        copies, axes, split_axis=0, concat_axis=0, tiled=True, axis_index_groups=group_of(axes)
    )


def near(array):
    return pltpu.with_memory_space_constraint(array, pltpu.VMEM)


def call(body, outs, name, scratch=(), cost=COST):
    return pl.pallas_call(
        body,
        out_shape=[jax.ShapeDtypeStruct(shape, dtype) for shape, dtype in outs],
        scratch_shapes=list(scratch),
        name=name,
        cost_estimate=pl.CostEstimate(flops=cost, bytes_accessed=cost // 256, transcendentals=0),
        compiler_params=pltpu.CompilerParams(vmem_limit_bytes=24 << 20),
    )


def rows_dot(left, right):
    return lax.dot_general(left, right, (((1,), (1,)), ((), ())), preferred_element_type=F32)


def iota(shape, dim):
    return lax.broadcasted_iota(jnp.int32, shape, dim)


def block_gain(gain_ref, block):
    gains = gain_ref[...].astype(F32)
    rows = iota(gains.shape, 0)
    first = jnp.sum(jnp.where(rows == 2 * block, gains, 0.0), axis=0, keepdims=True)
    second = jnp.sum(jnp.where(rows == 2 * block + 1, gains, 0.0), axis=0, keepdims=True)
    return jnp.concatenate([first, second], axis=1)


def spread_body(tokens, out):
    rows = tokens[...].astype(F32)
    line = jnp.concatenate([rows[at : at + 1] for at in range(rows.shape[0])], axis=1)
    out[...] = jnp.broadcast_to(line[None], out.shape)


def project_body(got, gain, query_w, key_w, value_w, forget_w, first_out, parts_out, block_out):
    position = lax.axis_index("kv_0") * 4 + lax.axis_index("kv_1")
    head = lax.axis_index("z") * 2 + lax.axis_index("core")
    peers = got.shape[0]
    sequences = block_out.shape[0]
    columns = LANES // sequences
    lines = jnp.concatenate([got[peers - FIRST_TP :], got[: peers - FIRST_TP]], axis=0)
    spread = jnp.broadcast_to(lines, (peers, columns, LANES)).reshape(peers * columns, LANES)
    keep = (iota(spread.shape, 1) // sequences) == (iota(spread.shape, 0) % columns)
    fold = (iota((sequences, LANES), 1) % sequences) == iota((sequences, LANES), 0)
    block = rows_dot(
        jnp.where(fold, 1.0, 0.0).astype(BF16), jnp.where(keep, spread, 0.0).astype(BF16)
    )
    block_out[...] = block
    own = (block * block_gain(gain, position)).astype(BF16)
    query = rows_dot(own, query_w[...])
    key = rows_dot(own, key_w[...])
    value = rows_dot(own, value_w[...])
    width = block.shape[1]
    gate_rows = forget_w[:, pl.ds(pl.multiple_of(position * width, width), width)]
    gates = rows_dot(own, gate_rows)
    gate = jnp.sum(jnp.where(iota(gates.shape, 1) == head, gates, 0.0), axis=1, keepdims=True)
    squares = jnp.sum(block * block, axis=1, keepdims=True)
    lane = iota((sequences, LANES - HD), 1)
    rest = jnp.where(lane == 0, gate, jnp.where(lane == 1, squares, 0.0))
    line = jnp.concatenate([query, rest], axis=1)
    first_out[...] = jnp.broadcast_to(line[None], first_out.shape)
    parts_out[...] = jnp.concatenate([key, value], axis=1)


def pieces(column):
    high = column.astype(BF16).astype(F32)
    middle = (column - high).astype(BF16).astype(F32)
    return high, middle, column - high - middle


def attend_body(model_width, got, parts, pairs, gates, lengths, second_out, row_out):
    position = lax.axis_index("kv_0") * 4 + lax.axis_index("kv_1")
    sequences = parts.shape[0]
    count = gates.shape[2]
    line = jnp.sum(got[...], axis=0)
    scale = lax.rsqrt(line[:, HD + 1 : HD + 2] / model_width + EPSILON)
    query = (line[:, :HD] * scale).astype(BF16)
    forget = jax.nn.log_sigmoid(line[:, HD : HD + 1] * scale)
    wide = sequences * HD
    own_group = (iota((sequences, wide), 1) // HD) == iota((sequences, wide), 0)
    spread = jnp.concatenate([query.astype(F32)] * sequences, axis=1)
    spread = jnp.where(own_group, spread, 0.0).astype(BF16)
    keys = pairs[:, 0, 0].reshape(wide, count)
    raw = jnp.dot(spread, keys, preferred_element_type=F32)
    diagonal = iota((sequences, sequences), 0) == iota((sequences, sequences), 1)
    ends = jnp.broadcast_to(lengths[...].reshape(1, sequences), (sequences, sequences))
    ends = jnp.sum(jnp.where(diagonal, ends, 0), axis=1, keepdims=True) - position * count
    live = iota((sequences, count), 1) < ends
    scores = jnp.where(live, raw * HD ** (-0.5) + gates[:, 0, :], NEG_FILL)
    top = jnp.max(scores, axis=1, keepdims=True)
    weights = jnp.where(live, jnp.exp(scores - top), 0.0)
    total = jnp.sum(weights, axis=1, keepdims=True)
    values = pairs[:, 0, 1].reshape(wide, count)
    sums = jnp.where(own_group, rows_dot(weights.astype(BF16), values), 0.0)
    folded = sums[:, :LANES]
    for at in range(LANES, wide, LANES):
        folded = folded + sums[:, at : at + LANES]
    block_sum = folded[:, :HD] + folded[:, HD:]
    own = jnp.sum(query.astype(F32) * parts[:, :HD], axis=1, keepdims=True)
    lane = iota((sequences, LANES), 1)
    stats = jnp.zeros((sequences, LANES), F32)
    for at, piece in enumerate((*pieces(top), *pieces(total), *pieces(own))):
        stats = jnp.where(lane == at, piece, stats)
    out = jnp.concatenate([block_sum, parts[:, HD:], stats], axis=1).astype(BF16)
    second_out[...] = jnp.broadcast_to(out[None], second_out.shape)
    row_out[...] = jnp.where(lane == 0, forget, jnp.where(lane == 1, scale, 0.0))


def combine_body(got, row, output_w, out):
    sums = got[:, :, :HD].astype(F32)
    value_parts = got[:, :, HD:LANES].astype(F32)
    stats = got[:, :, LANES:].astype(F32)
    forget, scale = row[:, 0:1], row[:, 1:2]

    def stat(at):
        return stats[:, :, at : at + 1] + stats[:, :, at + 1 : at + 2] + stats[:, :, at + 2 : at + 3]

    tops = stat(0) + forget[None]
    own_score = jnp.sum(stat(6), axis=0) * scale * HD ** (-0.5)
    value_new = (jnp.sum(value_parts, axis=0) * scale).astype(BF16).astype(F32)
    highest = jnp.maximum(jnp.max(tops, axis=0), own_score)
    factors = jnp.exp(tops - highest[None])
    own_factor = jnp.exp(own_score - highest)
    numerator = jnp.sum(factors * sums, axis=0) + own_factor * value_new
    denominator = jnp.sum(factors * stat(3), axis=0) + own_factor
    attended = (numerator / denominator).astype(BF16)
    projected = jnp.dot(attended, output_w[...], preferred_element_type=F32)
    out[...] = jnp.broadcast_to(projected.astype(BF16)[None], out.shape)


def mix_body(own, other, block, gain, up_w, third_out, middle_out):
    position = lax.axis_index("kv_0") * 4 + lax.axis_index("kv_1")
    middle = (block[...] + (own[...] + other[...])).astype(BF16)
    middle_out[...] = middle
    wide = middle.astype(F32)
    scaled = (wide * block_gain(gain, position)).astype(BF16)
    hidden = rows_dot(scaled, up_w[...])
    squares = jnp.sum(wide * wide, axis=1, keepdims=True)
    sequences, units = hidden.shape
    diagonal = iota((sequences, LANES), 0) == iota((sequences, LANES), 1)
    across = jnp.sum(jnp.where(diagonal, squares, 0.0), axis=0, keepdims=True)
    row = iota((8, LANES), 0)
    stats = jnp.zeros(row.shape, F32)
    for at, piece in enumerate(pieces(across)):
        stats = jnp.where(row == at, piece, stats)
    parts = [hidden[:, at : at + LANES] for at in range(0, units, LANES)]
    out = jnp.concatenate([*parts, stats], axis=0).astype(BF16)
    third_out[...] = jnp.broadcast_to(out[None], third_out.shape)


def down_body(model_width, got, down_w, out, turned):
    summed = jnp.sum(got[...].astype(F32), axis=0)
    sequences = turned.shape[1]
    units = down_w.shape[0] // LANES * sequences
    parts = [summed[at : at + sequences] for at in range(0, units, sequences)]
    across = jnp.sum(summed[units : units + 3], axis=0, keepdims=True)
    diagonal = iota((sequences, LANES), 0) == iota((sequences, LANES), 1)
    squares = jnp.sum(jnp.where(diagonal, across, 0.0), axis=1, keepdims=True)
    scale = lax.rsqrt(squares / model_width + EPSILON)
    activated = [jnp.square(jax.nn.relu(part * scale)).astype(BF16) for part in parts]
    activated = jnp.concatenate(activated, axis=1)
    down = jnp.dot(activated, down_w[...], preferred_element_type=F32)
    turned[...] = down.T
    peers = out.shape[0]
    columns = LANES // sequences
    lines = [turned[pl.ds(at, peers, stride=columns), :] for at in range(columns)]
    lines = jnp.concatenate(lines, axis=1).reshape(out.shape)
    out[...] = jnp.concatenate([lines[FIRST_TP:], lines[:FIRST_TP]], axis=0)


def finish_body(got, middle, out):
    head = lax.axis_index("z") * 2 + lax.axis_index("core")
    columns, sequences = out.shape
    line = jnp.sum(got[...], axis=0)
    own_shape = (columns, middle.shape[1])
    chosen = iota(own_shape, 1) == iota(own_shape, 0) + head * columns
    own = rows_dot(jnp.where(chosen, 1.0, 0.0).astype(BF16), middle[...])
    down = jnp.concatenate(
        [line[:, at * sequences : (at + 1) * sequences] for at in range(columns)], axis=0
    )
    out[...] = (own + down).astype(BF16)


def local(
    tokens,
    attention_gain,
    query_weight,
    key_weight,
    value_weight,
    forget_weight,
    cached_pairs,
    cached_gates,
    lengths,
    output_weight,
    mixer_gain,
    up_weight,
    down_weight,
):
    sequences, own_columns = tokens.shape
    blocks, heads = lax.axis_size(KV), lax.axis_size(TP)
    width = query_weight.shape[1]
    model_width = width * blocks
    hidden_units = up_weight.shape[0]

    (line,) = call(spread_body, [((heads, 1, sequences * own_columns), F32)], "spread")(tokens.T)
    got = exchange(line, TP)
    first, parts, block = call(
        project_body,
        [((blocks, sequences, LANES), F32), ((sequences, LANES), F32), ((sequences, width), F32)],
        "project",
        cost=1 << 20,
    )(
        got,
        near(attention_gain.reshape(-1, LANES)),
        near(query_weight),
        near(key_weight),
        near(value_weight),
        near(forget_weight),
    )
    got = exchange(first, KV)
    second, row = call(
        functools.partial(attend_body, model_width),
        [((blocks, sequences, 2 * LANES), BF16), ((sequences, LANES), F32)],
        "attend",
    )(got, parts, near(cached_pairs), near(cached_gates), near(lengths))
    got = exchange(second, KV)
    (projected,) = call(
        combine_body, [((lax.axis_size("z"), sequences, width), BF16)], "combine"
    )(got, row, near(output_weight))
    own = jnp.sum(exchange(projected, "z").astype(F32), axis=0)
    other = lax.ppermute(own, "core", [(0, 1), (1, 0)])
    third, middle = call(
        mix_body,
        [((blocks, sequences * hidden_units // LANES + 8, LANES), BF16), ((sequences, width), BF16)],
        "mix",
    )(own, other, block, near(mixer_gain.reshape(-1, LANES)), near(up_weight))
    got = exchange(third, KV)
    (down,) = call(
        functools.partial(down_body, model_width),
        [((heads, 1, LANES), F32)],
        "down",
        [pltpu.VMEM((width, sequences), F32)],
    )(got, near(down_weight))
    got = exchange(down, TP)
    (out,) = call(finish_body, [((own_columns, sequences), BF16)], "finish")(got, middle)
    return out.T


def solution(mesh):
    split = Mesh(mesh.devices.reshape(4, 4, 16, 2), KV_TP)
    return jax.shard_map(
        local,
        mesh=split,
        in_specs=(
            P(None, KV_TP),
            P(),
            P(TP, KV),
            P(TP, KV),
            P(TP, KV),
            P(),
            P(None, TP, None, None, KV),
            P(None, TP, KV),
            P(),
            P(TP, KV),
            P(),
            P(TP, KV),
            P(TP, KV),
        ),
        out_specs=P(None, KV_TP),
        check_vma=False,
    )
```

```python
import functools

import jax
import jax.numpy as jnp
import numpy as np
from jax import lax
from jax.experimental import pallas as pl
from jax.experimental.pallas import tpu as pltpu
from jax.sharding import Mesh
from jax.sharding import PartitionSpec as P

HD = 64
KV = ("kv_0", "kv_1")
TP = ("z", "core")
KV_TP = (*KV, *TP)
LANES = 128

COST = 1 << 34
EPSILON = 1e-06
NEG_FILL = -1e30
F32 = jnp.float32
BF16 = jnp.bfloat16


FIRST_Z, FIRST_TP = 10, 21


def group_of(axes):
    if axes == KV:
        row, column = np.divmod(np.arange(16), 4)
        order = (row + 2 * column + 2) % 4 * 4 + (column + 2) % 4
    elif axes == TP:
        order = np.roll(np.arange(32), -FIRST_TP)
    else:
        order = (FIRST_Z + 3 * np.arange(16)) % 16
    return [[int(index) for index in order.reshape(-1)]]


def exchange(copies, axes):
    return lax.all_to_all(
        copies, axes, split_axis=0, concat_axis=0, tiled=True, axis_index_groups=group_of(axes)
    )


def near(array):
    return pltpu.with_memory_space_constraint(array, pltpu.VMEM)


def call(body, outs, name, scratch=(), cost=COST):
    return pl.pallas_call(
        body,
        out_shape=[jax.ShapeDtypeStruct(shape, dtype) for shape, dtype in outs],
        scratch_shapes=list(scratch),
        name=name,
        cost_estimate=pl.CostEstimate(flops=cost, bytes_accessed=cost // 256, transcendentals=0),
        compiler_params=pltpu.CompilerParams(vmem_limit_bytes=24 << 20),
    )


def rows_dot(left, right):
    return lax.dot_general(left, right, (((1,), (1,)), ((), ())), preferred_element_type=F32)


def iota(shape, dim):
    return lax.broadcasted_iota(jnp.int32, shape, dim)


def block_gain(gain_ref, block):
    gains = gain_ref[...].astype(F32)
    rows = iota(gains.shape, 0)
    first = jnp.sum(jnp.where(rows == 2 * block, gains, 0.0), axis=0, keepdims=True)
    second = jnp.sum(jnp.where(rows == 2 * block + 1, gains, 0.0), axis=0, keepdims=True)
    return jnp.concatenate([first, second], axis=1)


def spread_body(tokens, out):
    rows = tokens[...].astype(F32)
    line = jnp.concatenate([rows[at : at + 1] for at in range(rows.shape[0])], axis=1)
    out[...] = jnp.broadcast_to(line[None], out.shape)


def project_body(got, gain, query_w, key_w, value_w, forget_w, first_out, parts_out, block_out):
    position = lax.axis_index("kv_0") * 4 + lax.axis_index("kv_1")
    head = lax.axis_index("z") * 2 + lax.axis_index("core")
    peers = got.shape[0]
    sequences = block_out.shape[0]
    columns = LANES // sequences
    lines = jnp.concatenate([got[peers - FIRST_TP :], got[: peers - FIRST_TP]], axis=0)
    spread = jnp.broadcast_to(lines, (peers, columns, LANES)).reshape(peers * columns, LANES)
    keep = (iota(spread.shape, 1) // sequences) == (iota(spread.shape, 0) % columns)
    fold = (iota((sequences, LANES), 1) % sequences) == iota((sequences, LANES), 0)
    block = rows_dot(
        jnp.where(fold, 1.0, 0.0).astype(BF16), jnp.where(keep, spread, 0.0).astype(BF16)
    )
    block_out[...] = block
    own = (block * block_gain(gain, position)).astype(BF16)
    query = rows_dot(own, query_w[...])
    key = rows_dot(own, key_w[...])
    value = rows_dot(own, value_w[...])
    width = block.shape[1]
    gate_rows = forget_w[:, pl.ds(pl.multiple_of(position * width, width), width)]
    gates = rows_dot(own, gate_rows)
    gate = jnp.sum(jnp.where(iota(gates.shape, 1) == head, gates, 0.0), axis=1, keepdims=True)
    squares = jnp.sum(block * block, axis=1, keepdims=True)
    lane = iota((sequences, LANES - HD), 1)
    rest = jnp.where(lane == 0, gate, jnp.where(lane == 1, squares, 0.0))
    line = jnp.concatenate([query, rest], axis=1)
    first_out[...] = jnp.broadcast_to(line[None], first_out.shape)
    parts_out[...] = jnp.concatenate([key, value], axis=1)


def pieces(column):
    high = column.astype(BF16).astype(F32)
    middle = (column - high).astype(BF16).astype(F32)
    return high, middle, column - high - middle


def attend_body(model_width, got, parts, pairs, gates, lengths, second_out, row_out):
    position = lax.axis_index("kv_0") * 4 + lax.axis_index("kv_1")
    sequences = parts.shape[0]
    count = gates.shape[2]
    line = jnp.sum(got[...], axis=0)
    scale = lax.rsqrt(line[:, HD + 1 : HD + 2] / model_width + EPSILON)
    query = (line[:, :HD] * scale).astype(BF16)
    forget = jax.nn.log_sigmoid(line[:, HD : HD + 1] * scale)
    wide = sequences * HD
    own_group = (iota((sequences, wide), 1) // HD) == iota((sequences, wide), 0)
    spread = jnp.concatenate([query.astype(F32)] * sequences, axis=1)
    spread = jnp.where(own_group, spread, 0.0).astype(BF16)
    keys = pairs[:, 0, 0].reshape(wide, count)
    raw = jnp.dot(spread, keys, preferred_element_type=F32)
    diagonal = iota((sequences, sequences), 0) == iota((sequences, sequences), 1)
    ends = jnp.broadcast_to(lengths[...].reshape(1, sequences), (sequences, sequences))
    ends = jnp.sum(jnp.where(diagonal, ends, 0), axis=1, keepdims=True) - position * count
    live = iota((sequences, count), 1) < ends
    scores = jnp.where(live, raw * HD ** (-0.5) + gates[:, 0, :], NEG_FILL)
    top = jnp.max(scores, axis=1, keepdims=True)
    weights = jnp.where(live, jnp.exp(scores - top), 0.0)
    total = jnp.sum(weights, axis=1, keepdims=True)
    values = pairs[:, 0, 1].reshape(wide, count)
    sums = jnp.where(own_group, rows_dot(weights.astype(BF16), values), 0.0)
    folded = sums[:, :LANES]
    for at in range(LANES, wide, LANES):
        folded = folded + sums[:, at : at + LANES]
    block_sum = folded[:, :HD] + folded[:, HD:]
    own = jnp.sum(query.astype(F32) * parts[:, :HD], axis=1, keepdims=True)
    lane = iota((sequences, LANES), 1)
    stats = jnp.zeros((sequences, LANES), F32)
    for at, piece in enumerate((*pieces(top), *pieces(total), *pieces(own))):
        stats = jnp.where(lane == at, piece, stats)
    out = jnp.concatenate([block_sum, parts[:, HD:], stats], axis=1).astype(BF16)
    second_out[...] = jnp.broadcast_to(out[None], second_out.shape)
    row_out[...] = jnp.where(lane == 0, forget, jnp.where(lane == 1, scale, 0.0))


def combine_body(got, row, output_w, out):
    sums = got[:, :, :HD].astype(F32)
    value_parts = got[:, :, HD:LANES].astype(F32)
    stats = got[:, :, LANES:].astype(F32)
    forget, scale = row[:, 0:1], row[:, 1:2]

    def stat(at):
        return stats[:, :, at : at + 1] + stats[:, :, at + 1 : at + 2] + stats[:, :, at + 2 : at + 3]

    tops = stat(0) + forget[None]
    own_score = jnp.sum(stat(6), axis=0) * scale * HD ** (-0.5)
    value_new = (jnp.sum(value_parts, axis=0) * scale).astype(BF16).astype(F32)
    highest = jnp.maximum(jnp.max(tops, axis=0), own_score)
    factors = jnp.exp(tops - highest[None])
    own_factor = jnp.exp(own_score - highest)
    numerator = jnp.sum(factors * sums, axis=0) + own_factor * value_new
    denominator = jnp.sum(factors * stat(3), axis=0) + own_factor
    attended = (numerator / denominator).astype(BF16)
    projected = jnp.dot(attended, output_w[...], preferred_element_type=F32)
    out[...] = jnp.broadcast_to(projected.astype(BF16)[None], out.shape)


def mix_body(own, other, block, gain, up_w, third_out, middle_out):
    position = lax.axis_index("kv_0") * 4 + lax.axis_index("kv_1")
    middle = (block[...] + (own[...] + other[...])).astype(BF16)
    middle_out[...] = middle
    wide = middle.astype(F32)
    scaled = (wide * block_gain(gain, position)).astype(BF16)
    hidden = rows_dot(scaled, up_w[...])
    squares = jnp.sum(wide * wide, axis=1, keepdims=True)
    sequences, units = hidden.shape
    diagonal = iota((sequences, LANES), 0) == iota((sequences, LANES), 1)
    across = jnp.sum(jnp.where(diagonal, squares, 0.0), axis=0, keepdims=True)
    row = iota((8, LANES), 0)
    stats = jnp.zeros(row.shape, F32)
    for at, piece in enumerate(pieces(across)):
        stats = jnp.where(row == at, piece, stats)
    parts = [hidden[:, at : at + LANES] for at in range(0, units, LANES)]
    out = jnp.concatenate([*parts, stats], axis=0).astype(BF16)
    third_out[...] = jnp.broadcast_to(out[None], third_out.shape)


def down_body(model_width, got, down_w, out, turned):
    summed = jnp.sum(got[...].astype(F32), axis=0)
    sequences = turned.shape[1]
    units = down_w.shape[0] // LANES * sequences
    parts = [summed[at : at + sequences] for at in range(0, units, sequences)]
    across = jnp.sum(summed[units : units + 3], axis=0, keepdims=True)
    diagonal = iota((sequences, LANES), 0) == iota((sequences, LANES), 1)
    squares = jnp.sum(jnp.where(diagonal, across, 0.0), axis=1, keepdims=True)
    scale = lax.rsqrt(squares / model_width + EPSILON)
    activated = [jnp.square(jax.nn.relu(part * scale)).astype(BF16) for part in parts]
    activated = jnp.concatenate(activated, axis=1)
    down = jnp.dot(activated, down_w[...], preferred_element_type=F32)
    turned[...] = down.T
    peers = out.shape[0]
    columns = LANES // sequences
    lines = [turned[pl.ds(at, peers, stride=columns), :] for at in range(columns)]
    lines = jnp.concatenate(lines, axis=1).reshape(out.shape)
    out[...] = jnp.concatenate([lines[FIRST_TP:], lines[:FIRST_TP]], axis=0)


def finish_body(got, middle, out):
    head = lax.axis_index("z") * 2 + lax.axis_index("core")
    columns, sequences = out.shape
    line = jnp.sum(got[...], axis=0)
    own_shape = (columns, middle.shape[1])
    chosen = iota(own_shape, 1) == iota(own_shape, 0) + head * columns
    own = rows_dot(jnp.where(chosen, 1.0, 0.0).astype(BF16), middle[...])
    down = jnp.concatenate(
        [line[:, at * sequences : (at + 1) * sequences] for at in range(columns)], axis=0
    )
    out[...] = (own + down).astype(BF16)


def local(
    tokens,
    attention_gain,
    query_weight,
    key_weight,
    value_weight,
    forget_weight,
    cached_pairs,
    cached_gates,
    lengths,
    output_weight,
    mixer_gain,
    up_weight,
    down_weight,
):
    sequences, own_columns = tokens.shape
    blocks, heads = lax.axis_size(KV), lax.axis_size(TP)
    width = query_weight.shape[1]
    model_width = width * blocks
    hidden_units = up_weight.shape[0]

    (line,) = call(spread_body, [((heads, 1, sequences * own_columns), F32)], "spread")(tokens.T)
    got = exchange(line, TP)
    first, parts, block = call(
        project_body,
        [((blocks, sequences, LANES), F32), ((sequences, LANES), F32), ((sequences, width), F32)],
        "project",
        cost=1 << 20,
    )(
        got,
        near(attention_gain.reshape(-1, LANES)),
        near(query_weight),
        near(key_weight),
        near(value_weight),
        near(forget_weight),
    )
    got = exchange(first, KV)
    second, row = call(
        functools.partial(attend_body, model_width),
        [((blocks, sequences, 2 * LANES), BF16), ((sequences, LANES), F32)],
        "attend",
    )(got, parts, near(cached_pairs), near(cached_gates), near(lengths))
    got = exchange(second, KV)
    (projected,) = call(
        combine_body, [((lax.axis_size("z"), sequences, width), BF16)], "combine"
    )(got, row, near(output_weight))
    own = jnp.sum(exchange(projected, "z").astype(F32), axis=0)
    other = lax.ppermute(own, "core", [(0, 1), (1, 0)])
    third, middle = call(
        mix_body,
        [((blocks, sequences * hidden_units // LANES + 8, LANES), BF16), ((sequences, width), BF16)],
        "mix",
    )(own, other, block, near(mixer_gain.reshape(-1, LANES)), near(up_weight))
    got = exchange(third, KV)
    (down,) = call(
        functools.partial(down_body, model_width),
        [((heads, 1, LANES), F32)],
        "down",
        [pltpu.VMEM((width, sequences), F32)],
    )(got, near(down_weight))
    got = exchange(down, TP)
    (out,) = call(finish_body, [((own_columns, sequences), BF16)], "finish")(got, middle)
    return out.T


def solution(mesh):
    split = Mesh(mesh.devices.reshape(4, 4, 16, 2), KV_TP)
    return jax.shard_map(
        local,
        mesh=split,
        in_specs=(
            P(None, KV_TP),
            P(),
            P(TP, KV),
            P(TP, KV),
            P(TP, KV),
            P(),
            P(None, TP, None, None, KV),
            P(None, TP, KV),
            P(),
            P(TP, KV),
            P(),
            P(TP, KV),
            P(TP, KV),
        ),
        out_specs=P(None, KV_TP),
        check_vma=False,
    )
```
